256 devices in a mesh: sp: 64 (over z, x, core), tp: 4 (over y).
Axes of the slice: x: 4, y: 4, z: 8, core: 2. Of those that a mesh axis runs over, the one named last changes fastest.
Arguments:
- hidden_in: bfloat16 [16384, 2048], P('sp'), may hold values from -6 to 6
- cotangent: bfloat16 [16384, 2048], P('sp'), may hold values from -16 to 16
- routes: int32 [16384, 2], P('sp'), may hold values from 0 to 63, all different within a row; in each aligned block of 256 rows (0 to 255, 256 to 511, ...) at most 12 rows name the same one
- routing_weights: float32 [16384, 2], P('sp'), may hold values from 0.1 to 1
- w_gate: bfloat16 [64, 2048, 1024], P('sp', None, 'tp'), may hold values from -0.125 to 0.125
- w_up: bfloat16 [64, 2048, 1024], P('sp', None, 'tp'), may hold values from -0.125 to 0.125
- w_down: bfloat16 [64, 1024, 2048], P('sp', 'tp'), may hold values from -0.1875 to 0.1875
- b_gate: bfloat16 [16384, 1024], P('sp', 'tp'), may hold values from -6 to 6
- c_gate: bfloat16 [16384, 1024], P('sp', 'tp'), may hold values from -6 to 6
- x_in: bfloat16 [16384, 1024], P('sp', 'tp'), may hold values from -6 to 6
- taps: bfloat16 [3, 1024], P(None, 'tp'), may hold values from -3 to 3
- w_out: bfloat16 [2048, 1024], P(None, 'tp'), may hold values from -0.1875 to 0.1875
Outputs:
- grad_gate: bfloat16 [64, 2048, 1024], P('sp', None, 'tp')
- grad_up: bfloat16 [64, 2048, 1024], P('sp', None, 'tp')
- grad_down: bfloat16 [64, 1024, 2048], P('sp', 'tp')
- out_proj_grad: float32 [2048, 1024], P('sp', 'tp')
- residual_grad: bfloat16 [16384, 2048], P('sp', 'tp')
- grad_b: bfloat16 [16384, 1024], P('sp', 'tp')
- grad_c: bfloat16 [16384, 1024], P('sp', 'tp')
- grad_x: bfloat16 [16384, 1024], P('sp', 'tp')
The draws below stay inside these ranges and needn't reach their ends.
Inputs may be any that keep to these rules, and one draw needn't show every extreme that they name: `routes`: each row names 2 different experts. Among the rows of one index of sp no expert is named more than 12 times, a bound that some block reaches in some of them.
All inputs are finite; a program needn't handle non-finite values.
Results may differ from the reference program's by a relative error of at most 0.01.
Values may be sent and summed in bfloat16 or wider, within the bound.
No kernel may reach another device: no remote copies, remote signals or barrier semaphores. Data moves between devices by JAX's collectives and lax.ppermute only.
A program may use at most 64 MiB of HBM per device.

```python
import math
import jax
import jax.numpy as jnp
import numpy as np
from jax import lax

D = 2048
SHORT = 1024
FF = 1024
TOP = 2
TOK_DEV = 256
EXPERTS = 64
CAP = 12
TOKENS = 16384
N_SP = 64
N_TP = 4


def spiked(entries, key, source, target, blocks, factor):
    owner, partner = [(jnp.arange(entries.shape[dim]) // (entries.shape[dim] // blocks)).reshape([-1 if axis == dim else 1 for axis in range(entries.ndim)]) for dim in (source, target)]
    chosen = jax.random.permutation(key, blocks)[partner]
    strong = (owner == chosen) | (owner == (partner + blocks // 2) % blocks)
    return jnp.where(strong, factor * entries, entries)


def shard_levels(own_key, shape, cuts, smallest, largest):
    def one(dim, shards_of):
        heights = jax.random.uniform(jax.random.fold_in(jax.random.fold_in(own_key, 6), dim), (shards_of,), jnp.float32, smallest / len(cuts), largest / len(cuts))
        return jnp.repeat(jnp.exp(heights), shape[dim] // shards_of).reshape((-1,) + (1,) * (len(shape) - dim - 1))

    factor_of = one(*cuts[0])
    for cut in cuts[1:]:
        factor_of = factor_of * one(*cut)
    return factor_of


def routed_block(rng, own, number, rows, amount, top, bound, skew):
    order = jax.random.permutation(rng, amount)
    crowded, ordinary = load_shares(amount, rows * top, bound, skew, True), load_shares(amount, rows * top, bound, skew, False)
    places = jnp.arange(amount)

    def named(sizes, rotation):
        used = int((sizes > 0).sum())
        fixed = max(1, used // 4)
        passed = fixed + (places - fixed + rotation * (used - fixed)) % max(1, amount - fixed)
        return jnp.zeros((amount,), jnp.int32).at[order[jnp.where(places < fixed, places, passed)]].set(jnp.asarray(sizes, jnp.int32))

    sizes = jnp.where(number % 4 == 0, named(crowded, number // 4), named(ordinary, number - number // 4 - 1))
    mixed = jax.random.permutation(jax.random.fold_in(own, 3), amount)
    donor, receiver = mixed[0:amount // 2 * 2:2], mixed[1:amount // 2 * 2:2]
    room = jnp.minimum(sizes[donor] - 1, bound - sizes[receiver]) // 2
    room = jnp.where((donor == order[0]) | (receiver == order[0]) | (sizes[receiver] == 0), 0, jnp.maximum(room, 0))
    passed = jax.random.randint(jax.random.fold_in(own, 4), (amount // 2,), 0, 1 << 20) % (room + 1)
    sizes = sizes.at[donor].add(-passed).at[receiver].add(passed)
    members = jnp.searchsorted(jnp.cumsum(sizes), jnp.arange(rows * top), side="right").astype(jnp.int32)
    table = members.reshape(top, rows).T
    table = table[jax.random.permutation(jax.random.fold_in(own, 1), rows)]
    rotation = jax.random.randint(jax.random.fold_in(own, 2), (rows, 1), 0, top)
    return jnp.take_along_axis(table, (jnp.arange(top)[None, :] + rotation) % top, axis=1)


def load_shares(number_of, total, bound, slope, full):
    weights = [(1 << 20) // math.isqrt(grade ** slope) + 1 for grade in range(1, number_of + 1)]
    largest = bound if full else min(bound, max(-(-total // number_of), total * weights[0] // sum(weights)))
    least = 1 if total - largest >= number_of - 1 else 0
    given, rest = [largest] + [least] * (number_of - 1), total - largest - least * (number_of - 1)
    while rest > 0:
        candidates = [i for i in range(1, number_of) if given[i] < largest] or [i for i in range(1, number_of) if given[i] < bound]
        mass, left = sum([weights[i] for i in candidates]), rest
        for i in candidates:
            more = min(bound - given[i], max(1, left * weights[i] // mass), rest)
            given[i] = given[i] + more
            rest = rest - more
    return np.array(given)


def bell_draw(key, dims, spread, limit, cuts=(), kind=jnp.bfloat16):
    entries = spread * jax.random.normal(key, dims, jnp.float32)
    if cuts:
        entries = entries * shard_levels(key, dims, cuts, -0.22, 0.18)
    return jnp.clip(entries, -limit, limit).astype(kind)


def noise_with(key, dims, deviation, limit, shards, heavy, kind=jnp.bfloat16):
    array = deviation * jax.random.normal(key, dims, jnp.float32)
    if shards:
        array = array * shard_levels(key, dims, shards, -0.22, 0.18)
    return jnp.clip(spiked(array, jax.random.fold_in(key, 3), *heavy), -limit, limit).astype(kind)


def setup_inputs(seed: int = 0) -> dict:
    streams_of = jax.random.split(jax.random.key(seed), 13)
    hidden_in = bell_draw(streams_of[0], (TOKENS, D), 1.0, 6.0, ((0, 64),))
    cotangent = noise_with(streams_of[1], (TOKENS, D), 1.0, 16.0, ((0, 64),), (0, 1, 64, 4.0))
    routes_keys = jax.random.split(jax.random.fold_in(streams_of[2], 1), TOKENS // TOK_DEV)
    routes_turns = jax.random.permutation(jax.random.fold_in(streams_of[2], 3), TOKENS // TOK_DEV)
    routes = jax.vmap(lambda own, number: routed_block(jax.random.fold_in(streams_of[2], 2), own, number, TOK_DEV, EXPERTS, TOP, CAP, 1))(routes_keys, routes_turns).reshape((TOKENS, TOP))
    routing_weights = jnp.clip(jnp.exp(math.log(1.0) - 2.3025851 * jax.random.uniform(streams_of[3], (TOKENS, TOP), jnp.float32) ** shard_levels(streams_of[3], (TOKENS, TOP), ((0, 64),), -0.2, 0.2)), 0.1, 1.0)
    w_gate = bell_draw(streams_of[4], (EXPERTS, D, FF), D ** -0.5, 0.125, ((0, 64), (2, 4)))
    w_up = bell_draw(streams_of[5], (EXPERTS, D, FF), D ** -0.5, 0.125, ((0, 64), (2, 4)))
    w_down = bell_draw(streams_of[6], (EXPERTS, FF, D), FF ** -0.5, 0.1875, ((0, 64), (1, 4)))
    b_gate = bell_draw(streams_of[7], (TOKENS, SHORT), 1.0, 6.0, ((0, 64), (1, 4)))
    c_gate = bell_draw(streams_of[8], (TOKENS, SHORT), 1.0, 6.0, ((0, 64), (1, 4)))
    x_in = bell_draw(streams_of[9], (TOKENS, SHORT), 1.0, 6.0, ((0, 64), (1, 4)))
    taps = bell_draw(streams_of[10], (3, SHORT), 0.6, 3.0, ((1, 4),))
    w_out = bell_draw(streams_of[11], (D, SHORT), SHORT ** -0.5, 0.1875, ((1, 4),))
    return {"hidden_in": hidden_in, "cotangent": cotangent, "routes": routes, "routing_weights": routing_weights, "w_gate": w_gate, "w_up": w_up, "w_down": w_down, "b_gate": b_gate, "c_gate": c_gate, "x_in": x_in, "taps": taps, "w_out": w_out}


def reference(hidden_in, cotangent, routes, routing_weights, w_gate, w_up, w_down, b_gate, c_gate, x_in, taps, w_out):
    flat_ids = routes.reshape(-1).astype(jnp.int32)
    flat_weights = routing_weights.reshape(-1).astype(jnp.float32)
    rows_each = N_SP * CAP
    part_width = FF // N_TP

    def one_expert(args):
        expert_id, gate_mat, up_mat, down_mat = args
        chosen = flat_ids == expert_id
        picked = jnp.nonzero(chosen, size=rows_each, fill_value=0)[0].astype(jnp.int32)
        filled = jnp.arange(rows_each, dtype=jnp.int32) < jnp.sum(chosen.astype(jnp.int32))
        token_of = picked // TOP
        rows_h = jnp.where(filled[:, None], hidden_in[token_of], jnp.zeros((), jnp.bfloat16))
        scaled = jnp.where(filled, flat_weights[picked], 0.0)
        rows_s = (scaled[:, None] * cotangent[token_of].astype(jnp.float32)).astype(jnp.bfloat16)
        pre_gate = jnp.dot(rows_h, gate_mat, preferred_element_type=jnp.float32)
        pre_up = jnp.dot(rows_h, up_mat, preferred_element_type=jnp.float32)
        sigma = jax.nn.sigmoid(pre_gate)
        silu_gate = pre_gate * sigma
        hid = (silu_gate * pre_up).astype(jnp.bfloat16)
        d_hid = jnp.dot(rows_s, down_mat.T, preferred_element_type=jnp.float32)
        d_up = (d_hid * silu_gate).astype(jnp.bfloat16)
        d_pre = (d_hid * pre_up * sigma * (1.0 + pre_gate * (1.0 - sigma))).astype(jnp.bfloat16)
        grad_down_e = jnp.dot(hid.T, rows_s, preferred_element_type=jnp.float32).astype(jnp.bfloat16)
        grad_gate_e = jnp.dot(rows_h.T, d_pre, preferred_element_type=jnp.float32).astype(jnp.bfloat16)
        grad_up_e = jnp.dot(rows_h.T, d_up, preferred_element_type=jnp.float32).astype(jnp.bfloat16)
        total = jnp.zeros((rows_each, D), jnp.float32)
        for block in range(N_TP):
            lower = block * part_width
            upper = lower + part_width
            partial_sum = jnp.dot(d_pre[:, lower:upper], gate_mat[:, lower:upper].T, preferred_element_type=jnp.float32)
            partial_sum = partial_sum + jnp.dot(d_up[:, lower:upper], up_mat[:, lower:upper].T, preferred_element_type=jnp.float32)
            total = total + partial_sum.astype(jnp.bfloat16).astype(jnp.float32)
        route_grad = jnp.where(filled[:, None], total.astype(jnp.bfloat16), jnp.zeros((), jnp.bfloat16))
        return grad_gate_e, grad_up_e, grad_down_e, route_grad, token_of

    expert_ids = jnp.arange(EXPERTS, dtype=jnp.int32)
    grad_gate, grad_up, grad_down, route_grads, token_ids = lax.map(one_expert, (expert_ids, w_gate, w_up, w_down))
    summed = jnp.zeros((TOKENS, D), jnp.float32).at[token_ids.reshape(-1)].add(route_grads.reshape(-1, D).astype(jnp.float32))
    residual_grad = (cotangent.astype(jnp.float32) + summed).astype(jnp.bfloat16)

    taps_f = taps.astype(jnp.float32)
    gated = c_gate.astype(jnp.float32) * x_in.astype(jnp.float32)
    padded = jnp.concatenate([jnp.zeros((2, SHORT), jnp.float32), gated], axis=0)
    conv = taps_f[0] * padded[0:TOKENS] + taps_f[1] * padded[1:TOKENS + 1] + taps_f[2] * padded[2:TOKENS + 2]
    b_f = b_gate.astype(jnp.float32)
    y_short = (b_f * conv).astype(jnp.bfloat16)
    d_y = jnp.dot(residual_grad, w_out, preferred_element_type=jnp.float32)
    grad_b = (d_y * conv).astype(jnp.bfloat16)
    d_conv = b_f * d_y
    later = jnp.concatenate([d_conv, jnp.zeros((2, SHORT), jnp.float32)], axis=0)
    d_v = taps_f[2] * later[0:TOKENS] + taps_f[1] * later[1:TOKENS + 1] + taps_f[0] * later[2:TOKENS + 2]
    grad_c = (d_v * x_in.astype(jnp.float32)).astype(jnp.bfloat16)
    grad_x = (d_v * c_gate.astype(jnp.float32)).astype(jnp.bfloat16)
    out_proj_grad = jnp.dot(residual_grad.T, y_short, preferred_element_type=jnp.float32)
    return grad_gate, grad_up, grad_down, out_proj_grad, residual_grad, grad_b, grad_c, grad_x
```

```python
import functools

import jax
import jax.numpy as jnp
from jax import lax
from jax.experimental import pallas as pl
from jax.experimental.pallas import tpu as pltpu
from jax.sharding import Mesh, PartitionSpec as P

BF = jnp.bfloat16
F32 = jnp.float32
SP = ("z", "x", "c")
MAIN = 8
VMEM_LIMIT = 56 * 1024 * 1024


def dot(a, b, contract):
    return lax.dot_general(a, b, ((contract[0], contract[1]), ((), ())), preferred_element_type=F32)


def nn(a, b):
    return dot(a, b, ((1,), (0,)))


def nt(a, b):
    return dot(a, b, ((1,), (1,)))


def tn(a, b):
    return dot(a, b, ((0,), (0,)))


def shifted(x, axis, by):
    n = lax.axis_size(axis)
    return lax.ppermute(x, axis, [(i, (i + by) % n) for i in range(n)])


def selection(row, base=0):
    n_rows = 64 * MAIN
    at = lax.broadcasted_iota(jnp.int32, (n_rows, row.shape[1]), 0)
    return at == (row + base)


def route_kernel(tp_ref, ids_ref, w_ref, h_ref, c_ref, out_ref, rows_ref):
    tokens = ids_ref.shape[1]
    expert = lax.broadcasted_iota(jnp.int32, (64, tokens), 0)
    upper = (
        lax.broadcasted_iota(jnp.int32, (tokens, tokens), 0)
        < lax.broadcasted_iota(jnp.int32, (tokens, tokens), 1)
    ).astype(F32).astype(BF)
    ids0, ids1 = ids_ref[0:1, :], ids_ref[1:2, :]
    hot0 = (expert == ids0).astype(F32)
    hot1 = (expert == ids1).astype(F32)
    before0 = nn(hot0.astype(BF), upper)
    before1 = nn(hot1.astype(BF), upper) + jnp.sum(hot0, axis=1, keepdims=True)
    pos0 = jnp.sum(hot0 * before0, axis=0, keepdims=True).astype(jnp.int32)
    pos1 = jnp.sum(hot1 * before1, axis=0, keepdims=True).astype(jnp.int32)
    w0, w1 = w_ref[0:1, :], w_ref[1:2, :]
    none = jnp.full_like(ids0, -64)
    a0 = jnp.where(pos0 < MAIN, ids0 * MAIN + pos0, none)
    a1 = jnp.where(pos1 < MAIN, ids1 * MAIN + pos1, none)
    b0 = jnp.where((pos0 >= MAIN) & (pos0 < MAIN + 4), ids0 * MAIN + pos0 - MAIN, none)
    b1 = jnp.where((pos1 >= MAIN) & (pos1 < MAIN + 4), ids1 * MAIN + pos1 - MAIN, none)
    rows_ref[0:1, :] = a0
    rows_ref[1:2, :] = a1
    rows_ref[2:3, :] = b0
    rows_ref[3:4, :] = b1
    h, c = h_ref[...], c_ref[...]
    width = h.shape[1]

    def picked(r0, r1, base):
        s0, s1 = selection(r0, base), selection(r1, base)
        weight = jnp.sum(jnp.where(s0, w0, 0.0) + jnp.where(s1, w1, 0.0), axis=1, keepdims=True)
        return (s0 | s1).astype(F32).astype(BF), weight

    sel, weight = picked(a0, a1, 0)
    out_ref[:, 0:width] = nn(sel, h).astype(BF)
    out_ref[:, width : 2 * width] = (nn(sel, c) * weight).astype(BF)
    sel_h, _ = picked(b0, b1, 0)
    sel_s, weight = picked(b0, b1, 4)
    out_ref[:, 2 * width : 3 * width] = (nn(sel_h, h) + nn(sel_s, c) * weight).astype(BF)


def route(tp, ids, weights, hidden_in, cotangent):
    tokens, width = hidden_in.shape[0], hidden_in.shape[1] // 4
    share = pl.BlockSpec((tokens, width), lambda i, t: (0, t[0]))
    whole = lambda shape: pl.BlockSpec(shape, lambda i, t: (0, 0))
    return pl.pallas_call(
        route_kernel,
        grid_spec=pltpu.PrefetchScalarGridSpec(
            num_scalar_prefetch=1,
            grid=(1,),
            in_specs=[whole(ids.shape), whole(weights.shape), share, share],
            out_specs=[whole((64 * MAIN, 3 * width)), whole((4, tokens))],
        ),
        out_shape=[
            jax.ShapeDtypeStruct((64 * MAIN, 3 * width), BF),
            jax.ShapeDtypeStruct((4, tokens), jnp.int32),
        ],
        compiler_params=pltpu.CompilerParams(vmem_limit_bytes=VMEM_LIMIT),
        name="route",
    )(tp, ids, weights, hidden_in, cotangent)


def combine_kernel(tp_ref, rows_ref, back_ref, c_ref, out_ref):
    width = c_ref.shape[1]
    a0, a1, b0, b1 = (rows_ref[k : k + 1, :] for k in range(4))

    def sel(r0, r1, base):
        return (selection(r0, base) | selection(r1, base)).astype(F32).astype(BF)

    main = tn(sel(a0, a1, 0), back_ref[:, 0:width])
    rest = back_ref[:, width:]
    low = tn(sel(b0, b1, 0), rest)
    high = tn(sel(b0, b1, 4), rest)
    half = width // 2
    out_ref[:, 0:half] = (c_ref[:, 0:half].astype(F32) + (main[:, 0:half] + low)).astype(BF)
    out_ref[:, half:] = (c_ref[:, half:].astype(F32) + (main[:, half:] + high)).astype(BF)


def combine(tp, rows, back, cotangent):
    tokens, width = cotangent.shape[0], cotangent.shape[1] // 4
    whole = lambda shape: pl.BlockSpec(shape, lambda i, t: (0, 0))
    return pl.pallas_call(
        combine_kernel,
        grid_spec=pltpu.PrefetchScalarGridSpec(
            num_scalar_prefetch=1,
            grid=(1,),
            in_specs=[
                whole(rows.shape),
                whole(back.shape),
                pl.BlockSpec((tokens, width), lambda i, t: (0, t[0])),
            ],
            out_specs=whole((tokens, width)),
        ),
        out_shape=jax.ShapeDtypeStruct((tokens, width), BF),
        compiler_params=pltpu.CompilerParams(vmem_limit_bytes=VMEM_LIMIT),
        name="combine",
    )(tp, rows, back, cotangent)


def block_at(tp, by):
    return lax.rem(tp + by, 4)


def expert_kernel(
    tp_ref, own_ref, prev_ref, next_ref, far_lo_ref, far_hi_ref, wg_ref, wu_ref, wd_ref,
    far_lo_out, far_hi_out, up_lo_out, up_hi_out, down_lo_out, down_hi_out, own_out, da_out, db_out,
    ga, ua, da, gb, ub, db,
):
    tp = tp_ref[0]
    n_rows = own_ref.shape[0]
    half = n_rows // 2
    width = own_ref.shape[1] // 3
    ff = wg_ref.shape[1]

    def rows_of(j):
        return pl.ds(pl.multiple_of(j * width, width), width)

    def add(ref, lo, x, first):
        if first:
            ref[lo : lo + x.shape[0], :] = x
        else:
            ref[lo : lo + x.shape[0], :] += x

    def take(x_ref, by, lo, first):
        j = block_at(tp, by)
        wg, wu, wd = wg_ref[rows_of(j), :], wu_ref[rows_of(j), :], wd_ref[:, rows_of(j)]
        h, s, m = x_ref[:, 0:width], x_ref[:, width : 2 * width], x_ref[:, 2 * width :]
        add(ga, lo, nn(h, wg), first)
        add(ua, lo, nn(h, wu), first)
        add(da, lo, nt(s, wd), first)
        add(gb, lo, nn(m, wg), first)
        add(ub, lo, nn(m, wu), first)
        add(db, lo, nt(m, wd), first)

    take(own_ref, 0, 0, True)
    take(prev_ref, 3, 0, False)
    take(next_ref, 1, 0, False)
    take(far_lo_ref, 2, 0, False)
    take(far_hi_ref, 2, half, False)

    def local(g, u, d):
        sigma = 1.0 / (1.0 + jnp.exp(-g))
        silu = g * sigma
        return d * u * sigma * (1.0 + g * (1.0 - sigma)), d * silu, silu * u

    p, q, r = local(ga[...], ua[...], da[...])
    da_out[:, 0:ff] = p.astype(BF)
    da_out[:, ff : 2 * ff] = q.astype(BF)
    da_out[:, 2 * ff :] = r.astype(BF)
    keep = lax.rem(lax.broadcasted_iota(jnp.int32, (n_rows, ff), 0), 8) < 4
    p, q, r = local(gb[...], ub[...], pltpu.roll(db[...], n_rows - 4, 0))
    p, q, r = (jnp.where(keep, v, 0.0) for v in (p, q, r))
    db_out[:, 0:ff] = p.astype(BF)
    db_out[:, ff : 2 * ff] = q.astype(BF)
    db_out[:, 2 * ff :] = pltpu.roll(r, 4, 0).astype(BF)
    high_p = pltpu.roll(p, 4, 0).astype(BF)
    high_q = pltpu.roll(q, 4, 0).astype(BF)

    def give(by, pieces):
        j = block_at(tp, by)
        wg, wu = wg_ref[rows_of(j), :], wu_ref[rows_of(j), :]
        cut = width // 2
        main = nt(da_out[:, 0:ff], wg) + nt(da_out[:, ff : 2 * ff], wu)
        rest = nt(db_out[:, 0:ff], wg[0:cut]) + nt(db_out[:, ff : 2 * ff], wu[0:cut])
        rest = rest + nt(high_p, wg[cut:]) + nt(high_q, wu[cut:])
        main, rest = main.astype(BF), rest.astype(BF)
        at = 0
        for ref in pieces:
            ref[:, 0:width] = main[at : at + ref.shape[0]]
            ref[:, width:] = rest[at : at + ref.shape[0]]
            at += ref.shape[0]

    give(2, (far_lo_out, far_hi_out))
    give(1, (up_lo_out, up_hi_out))
    give(3, (down_lo_out, down_hi_out))
    give(0, (own_out,))


def vmem_specs(n):
    return [pl.BlockSpec(memory_space=pltpu.VMEM) for _ in range(n)]


def expert(tp, blocks, wg, wu, wd):
    n_rows = blocks[0].shape[0]
    ff = wg.shape[1]
    width = blocks[0].shape[1] // 3
    half = jax.ShapeDtypeStruct((n_rows // 2, width + width // 2), BF)
    return pl.pallas_call(
        expert_kernel,
        in_specs=[pl.BlockSpec(memory_space=pltpu.SMEM)] + vmem_specs(8),
        out_specs=vmem_specs(9),
        out_shape=[half] * 6
        + [
            jax.ShapeDtypeStruct((n_rows, width + width // 2), BF),
            jax.ShapeDtypeStruct((n_rows, 3 * ff), BF),
            jax.ShapeDtypeStruct((n_rows, 3 * ff), BF),
        ],
        scratch_shapes=[pltpu.VMEM((n_rows, ff), F32)] * 6,
        compiler_params=pltpu.CompilerParams(vmem_limit_bytes=VMEM_LIMIT),
        name="expert",
    )(tp, *blocks, wg, wu, wd)


def weights_kernel(
    tp_ref, own_ref, prev_ref, next_ref, far_lo_ref, far_hi_ref, da_ref, db_ref, gg_ref, gu_ref, gd_ref
):
    tp = tp_ref[0]
    width = own_ref.shape[1] // 3
    half = own_ref.shape[0] // 2
    ff = gd_ref.shape[0]

    def sums(x_ref, lo):
        n = x_ref.shape[0]
        da, db = da_ref[lo : lo + n, :], db_ref[lo : lo + n, :]
        h, s, m = x_ref[:, 0:width], x_ref[:, width : 2 * width], x_ref[:, 2 * width :]
        both = tn(h, da[:, 0 : 2 * ff]) + tn(m, db[:, 0 : 2 * ff])
        down = tn(da[:, 2 * ff :], s) + tn(db[:, 2 * ff :], m)
        return both, down

    def put(by, both, down):
        at = pl.ds(pl.multiple_of(block_at(tp, by) * width, width), width)
        gg_ref[at, :] = both[:, 0:ff].astype(BF)
        gu_ref[at, :] = both[:, ff:].astype(BF)
        gd_ref[:, at] = down.astype(BF)

    put(0, *sums(own_ref, 0))
    put(3, *sums(prev_ref, 0))
    put(1, *sums(next_ref, 0))
    both, down = sums(far_lo_ref, 0)
    both_hi, down_hi = sums(far_hi_ref, half)
    put(2, both + both_hi, down + down_hi)


def weight_grads(tp, blocks, da, db):
    width = blocks[0].shape[1] // 3
    ff = da.shape[1] // 3
    return pl.pallas_call(
        weights_kernel,
        in_specs=[pl.BlockSpec(memory_space=pltpu.SMEM)] + vmem_specs(7),
        out_specs=vmem_specs(3),
        out_shape=[
            jax.ShapeDtypeStruct((4 * width, ff), BF),
            jax.ShapeDtypeStruct((4 * width, ff), BF),
            jax.ShapeDtypeStruct((ff, 4 * width), BF),
        ],
        compiler_params=pltpu.CompilerParams(vmem_limit_bytes=VMEM_LIMIT),
        name="weight_grads",
    )(tp, *blocks, da, db)


def mixer_kernel(
    where_ref, own_ref, prev_ref, next_ref, far_ref, wo_ref, conv_ref, y_ref, b_ref,
    gb_ref, dc_ref, mine_ref, other_ref,
):
    tp, core = where_ref[0], where_ref[1]
    width = own_ref.shape[1]
    y = y_ref[...]
    d_y = None
    for ref, by in ((own_ref, 0), (prev_ref, 3), (next_ref, 1), (far_ref, 2)):
        at = pl.multiple_of(block_at(tp, by) * width, width)
        part = nn(ref[...], wo_ref[pl.ds(at, width), :])
        d_y = part if d_y is None else d_y + part
        grad = tn(ref[...], y).astype(BF).reshape(width // 64, 2, 32, y.shape[1])
        low, high = grad[:, 0], grad[:, 1]
        shape = (width // 2, y.shape[1])
        to = pl.ds(pl.multiple_of(block_at(tp, by) * (width // 2), width // 2), width // 2)
        first = core == 0
        mine_ref[to, :] = jnp.where(first, low, high).reshape(shape)
        other_ref[to, :] = jnp.where(first, high, low).reshape(shape)
    gb_ref[...] = (d_y * conv_ref[...]).astype(BF)
    dc_ref[...] = b_ref[...].astype(F32) * d_y


def mixer(where, blocks, w_out, conv, y_short, b_gate):
    tokens, width = blocks[0].shape
    chan = w_out.shape[1]
    return pl.pallas_call(
        mixer_kernel,
        in_specs=[pl.BlockSpec(memory_space=pltpu.SMEM)] + vmem_specs(8),
        out_specs=vmem_specs(4),
        out_shape=[
            jax.ShapeDtypeStruct((tokens, chan), BF),
            jax.ShapeDtypeStruct((tokens, chan), F32),
            jax.ShapeDtypeStruct((2 * width, chan), BF),
            jax.ShapeDtypeStruct((2 * width, chan), BF),
        ],
        compiler_params=pltpu.CompilerParams(vmem_limit_bytes=VMEM_LIMIT),
        name="mixer",
    )(where, *blocks, w_out, conv, y_short, b_gate)


def from_behind(x, by):
    n = lax.axis_size(SP)
    return lax.ppermute(x, SP, [(i, i + by) for i in range(n) if 0 <= i + by < n])


def per_device(
    hidden_in, cotangent, routes, routing_weights, w_gate, w_up, w_down, b_gate, c_gate, x_in, taps, w_out
):
    tok_rows, model_width = hidden_in.shape
    share = model_width // 4
    y_at = lax.axis_index("y").astype(jnp.int32)
    tp = y_at.reshape(1)
    where = jnp.stack([y_at, lax.axis_index("c").astype(jnp.int32)])
    wg, wu, wd = w_gate[0], w_up[0], w_down[0]

    sent, rows = route(tp, routes.T, routing_weights.T, hidden_in, cotangent)
    own = lax.all_to_all(sent.reshape(64, MAIN, 3 * share), SP, split_axis=0, concat_axis=0, tiled=True)
    own = own.reshape(64 * MAIN, 3 * share)
    half = own.shape[0] // 2

    prev = shifted(own, "y", 1)
    after = shifted(own, "y", -1)
    far_lo = shifted(prev[:half], "y", 1)
    far_hi = shifted(after[half:], "y", -1)
    blocks = (own, prev, after, far_lo, far_hi)

    f_lo, f_hi, u_lo, u_hi, d_lo, d_hi, o, da, db = expert(tp, blocks, wg, wu, wd)

    from_prev = shifted(f_lo, "y", 1)
    from_next = shifted(f_hi, "y", -1)
    prev_hi = shifted(u_hi, "y", 1)
    next_lo = shifted(d_lo, "y", -1)
    added = lambda a, b: (a.astype(F32) + b.astype(F32)).astype(BF)
    prev_lo = shifted(added(u_lo, from_prev), "y", 1)
    next_hi = shifted(added(d_hi, from_next), "y", -1)
    got_prev = jnp.concatenate([prev_lo, prev_hi], axis=0).astype(F32)
    got_next = jnp.concatenate([next_lo, next_hi], axis=0).astype(F32)
    total = (o.astype(F32) + got_prev + got_next).astype(BF)
    back = lax.all_to_all(
        total.reshape(64, MAIN, total.shape[1]), SP, split_axis=0, concat_axis=0, tiled=True
    ).reshape(total.shape)

    residual_grad = combine(tp, rows, back, cotangent)
    res_blocks = (
        residual_grad,
        shifted(residual_grad, "y", 1),
        shifted(residual_grad, "y", -1),
        shifted(residual_grad, "y", 2),
    )

    taps_f = taps.astype(F32)
    gated = c_gate.astype(F32) * x_in.astype(F32)
    earlier = from_behind(gated[tok_rows - 2 :], 1)
    padded = jnp.concatenate([earlier, gated], axis=0)
    conv = (
        taps_f[0] * padded[0:tok_rows]
        + taps_f[1] * padded[1 : tok_rows + 1]
        + taps_f[2] * padded[2 : tok_rows + 2]
    )
    y_short = (b_gate.astype(F32) * conv).astype(BF)

    grad_b, d_conv, mine, other = mixer(where, res_blocks, w_out, conv, y_short, b_gate)
    following = from_behind(d_conv[0:2], -1)
    later = jnp.concatenate([d_conv, following], axis=0)
    d_v = (
        taps_f[2] * later[0:tok_rows]
        + taps_f[1] * later[1 : tok_rows + 1]
        + taps_f[0] * later[2 : tok_rows + 2]
    )
    grad_c = (d_v * x_in.astype(F32)).astype(BF)
    grad_x = (d_v * c_gate.astype(F32)).astype(BF)

    chip = added(mine, shifted(other, "c", 1)).reshape(32, 32, mine.shape[1])
    parts = lax.all_to_all(chip, ("z", "x"), split_axis=0, concat_axis=0, tiled=True)
    out_proj_grad = jnp.sum(parts.astype(F32), axis=0)

    gg, gu, gd = weight_grads(tp, blocks, da, db)
    return (gg[None], gu[None], gd[None], out_proj_grad, residual_grad, grad_b, grad_c, grad_x)


def solution(mesh):
    fine = Mesh(mesh.devices.reshape(8, 4, 2, 4), ("z", "x", "c", "y"))
    rows = P(SP, None)
    both = P(SP, "y")
    return jax.shard_map(
        per_device,
        mesh=fine,
        in_specs=(
            rows, rows, rows, rows,
            P(SP, None, "y"), P(SP, None, "y"), P(SP, "y", None),
            both, both, both, P(None, "y"), P(None, "y"),
        ),
        out_specs=(P(SP, None, "y"), P(SP, None, "y"), P(SP, "y", None), both, both, both, both, both),
        check_vma=False,
    )
```

```python
import jax
import jax.numpy as jnp
from jax import lax
from jax.experimental import pallas as pl
from jax.experimental.pallas import tpu as pltpu
from jax.sharding import Mesh, PartitionSpec as P

BF = jnp.bfloat16
F32 = jnp.float32
SP = ("z", "x", "c")
MAIN = 8
VMEM_LIMIT = 56 * 1024 * 1024


def dot(a, b, contract):
    return lax.dot_general(a, b, ((contract[0], contract[1]), ((), ())), preferred_element_type=F32)


def nn(a, b):
    return dot(a, b, ((1,), (0,)))


def nt(a, b):
    return dot(a, b, ((1,), (1,)))


def tn(a, b):
    return dot(a, b, ((0,), (0,)))


def shifted(x, axis, by):
    n = lax.axis_size(axis)
    return lax.ppermute(x, axis, [(i, (i + by) % n) for i in range(n)])


def selection(row, base=0):
    n_rows = 64 * MAIN
    at = lax.broadcasted_iota(jnp.int32, (n_rows, row.shape[1]), 0)
    return at == (row + base)


def route_kernel(tp_ref, ids_ref, w_ref, h_ref, c_ref, hd_ref, cd_ref, out_ref, direct_ref, rows_ref):
    tokens = ids_ref.shape[1]
    expert = lax.broadcasted_iota(jnp.int32, (64, tokens), 0)
    upper = (
        lax.broadcasted_iota(jnp.int32, (tokens, tokens), 0)
        < lax.broadcasted_iota(jnp.int32, (tokens, tokens), 1)
    ).astype(F32).astype(BF)
    ids0, ids1 = ids_ref[0:1, :], ids_ref[1:2, :]
    hot0 = (expert == ids0).astype(F32)
    hot1 = (expert == ids1).astype(F32)
    before0 = nn(hot0.astype(BF), upper)
    before1 = nn(hot1.astype(BF), upper) + jnp.sum(hot0, axis=1, keepdims=True)
    pos0 = jnp.sum(hot0 * before0, axis=0, keepdims=True).astype(jnp.int32)
    pos1 = jnp.sum(hot1 * before1, axis=0, keepdims=True).astype(jnp.int32)
    w0, w1 = w_ref[0:1, :], w_ref[1:2, :]
    none = jnp.full_like(ids0, -64)
    a0 = jnp.where(pos0 < MAIN, ids0 * MAIN + pos0, none)
    a1 = jnp.where(pos1 < MAIN, ids1 * MAIN + pos1, none)
    b0 = jnp.where((pos0 >= MAIN) & (pos0 < MAIN + 4), ids0 * MAIN + pos0 - MAIN, none)
    b1 = jnp.where((pos1 >= MAIN) & (pos1 < MAIN + 4), ids1 * MAIN + pos1 - MAIN, none)
    rows_ref[0:1, :] = a0
    rows_ref[1:2, :] = a1
    rows_ref[2:3, :] = b0
    rows_ref[3:4, :] = b1

    def picked(r0, r1, base):
        s0, s1 = selection(r0, base), selection(r1, base)
        weight = jnp.sum(jnp.where(s0, w0, 0.0) + jnp.where(s1, w1, 0.0), axis=1, keepdims=True)
        return (s0 | s1).astype(F32).astype(BF), weight

    sel, weight = picked(a0, a1, 0)
    sel_h, _ = picked(b0, b1, 0)
    sel_s, weight_s = picked(b0, b1, 4)
    for h_in, c_in, to in ((h_ref, c_ref, out_ref), (hd_ref, cd_ref, direct_ref)):
        h, c = h_in[...], c_in[...]
        width = h.shape[1]
        to[:, 0:width] = nn(sel, h).astype(BF)
        to[:, width : 2 * width] = (nn(sel, c) * weight).astype(BF)
        to[:, 2 * width :] = (nn(sel_h, h) + nn(sel_s, c) * weight_s).astype(BF)


def route(tp, ids, weights, hidden_in, cotangent):
    tokens, width = hidden_in.shape
    direct = width // 4
    ring = (width - direct) // 4
    share = pl.BlockSpec((tokens, ring), lambda i, t: (0, t[0]))
    last = pl.BlockSpec((tokens, direct), lambda i, t: (0, 3))
    whole = lambda shape: pl.BlockSpec(shape, lambda i, t: (0, 0))
    return pl.pallas_call(
        route_kernel,
        grid_spec=pltpu.PrefetchScalarGridSpec(
            num_scalar_prefetch=1,
            grid=(1,),
            in_specs=[whole(ids.shape), whole(weights.shape), share, share, last, last],
            out_specs=[whole((64 * MAIN, 3 * ring)), whole((64 * MAIN, 3 * direct)), whole((4, tokens))],
        ),
        out_shape=[
            jax.ShapeDtypeStruct((64 * MAIN, 3 * ring), BF),
            jax.ShapeDtypeStruct((64 * MAIN, 3 * direct), BF),
            jax.ShapeDtypeStruct((4, tokens), jnp.int32),
        ],
        compiler_params=pltpu.CompilerParams(vmem_limit_bytes=VMEM_LIMIT),
        name="route",
    )(tp, ids, weights, hidden_in, cotangent, hidden_in, cotangent)


def combine_kernel(tp_ref, rows_ref, back_ref, c_ref, out_ref):
    width = c_ref.shape[1]
    a0, a1, b0, b1 = (rows_ref[k : k + 1, :] for k in range(4))

    def sel(r0, r1, base):
        return (selection(r0, base) | selection(r1, base)).astype(F32).astype(BF)

    main = tn(sel(a0, a1, 0), back_ref[:, 0:width])
    rest = back_ref[:, width:]
    low = tn(sel(b0, b1, 0), rest)
    high = tn(sel(b0, b1, 4), rest)
    half = width // 2
    out_ref[:, 0:half] = (c_ref[:, 0:half].astype(F32) + (main[:, 0:half] + low)).astype(BF)
    out_ref[:, half:] = (c_ref[:, half:].astype(F32) + (main[:, half:] + high)).astype(BF)


def combine(tp, rows, back, cotangent):
    tokens, width = cotangent.shape[0], cotangent.shape[1] // 4
    whole = lambda shape: pl.BlockSpec(shape, lambda i, t: (0, 0))
    return pl.pallas_call(
        combine_kernel,
        grid_spec=pltpu.PrefetchScalarGridSpec(
            num_scalar_prefetch=1,
            grid=(1,),
            in_specs=[
                whole(rows.shape),
                whole(back.shape),
                pl.BlockSpec((tokens, width), lambda i, t: (0, t[0])),
            ],
            out_specs=whole((tokens, width)),
        ),
        out_shape=jax.ShapeDtypeStruct((tokens, width), BF),
        compiler_params=pltpu.CompilerParams(vmem_limit_bytes=VMEM_LIMIT),
        name="combine",
    )(tp, rows, back, cotangent)


def block_at(tp, by):
    return lax.rem(tp + by, 4)


def vmem_specs(n):
    return [pl.BlockSpec(memory_space=pltpu.VMEM) for _ in range(n)]


def local_call(kernel, scalars, arrays, outs, scratch=()):
    return pl.pallas_call(
        kernel,
        in_specs=[pl.BlockSpec(memory_space=pltpu.SMEM)] + vmem_specs(len(arrays)),
        out_specs=vmem_specs(len(outs)),
        out_shape=[jax.ShapeDtypeStruct(shape, dtype) for shape, dtype in outs],
        scratch_shapes=list(scratch),
        compiler_params=pltpu.CompilerParams(vmem_limit_bytes=VMEM_LIMIT),
    )(scalars, *arrays)


def block_rows(tp, by, width):
    return pl.ds(pl.multiple_of(block_at(tp, by) * width, width), width)


def gather_products(sums, lo, x_ref, wg, wu, wd, first):
    ga, ua, da, gb, ub, db = sums
    width = x_ref.shape[1] // 3
    to = slice(lo, lo + x_ref.shape[0])
    h, s, m = x_ref[:, 0:width], x_ref[:, width : 2 * width], x_ref[:, 2 * width :]

    def add(ref, x):
        ref[to, :] = x if first else ref[to, :] + x

    add(ga, nn(h, wg))
    add(ua, nn(h, wu))
    add(da, nt(s, wd))
    add(gb, nn(m, wg))
    add(ub, nn(m, wu))
    add(db, nt(m, wd))


def early_kernel(tp_ref, own_ref, prev_ref, next_ref, wg_ref, wu_ref, wd_ref, *sums):
    tp = tp_ref[0]
    width = own_ref.shape[1] // 3
    for ref, by in ((own_ref, 0), (prev_ref, 3), (next_ref, 1)):
        at = block_rows(tp, by, width)
        gather_products(sums, 0, ref, wg_ref[at, :], wu_ref[at, :], wd_ref[:, at], by == 0)


def partial_rows(da, db, high_p, high_q, wg, wu):
    ff = wg.shape[1]
    cut = wg.shape[0] // 2
    main = nt(da[:, 0:ff], wg) + nt(da[:, ff : 2 * ff], wu)
    rest = nt(db[:, 0:ff], wg[0:cut]) + nt(db[:, ff : 2 * ff], wu[0:cut])
    rest = rest + nt(high_p, wg[cut:]) + nt(high_q, wu[cut:])
    return main.astype(BF), rest.astype(BF)


def write_rows(refs, main, rest):
    at = 0
    for ref in refs:
        n, width = ref.shape[0], main.shape[1]
        ref[:, 0:width] = main[at : at + n]
        ref[:, width:] = rest[at : at + n]
        at += n


def late_kernel(
    tp_ref, ga_in, ua_in, da_in, gb_in, ub_in, db_in, far_lo_ref, far_hi_ref, direct_ref,
    wg_ref, wu_ref, wd_ref, da_out, db_out, far_lo_out, far_hi_out, ga, ua, da, gb, ub, db,
):
    tp = tp_ref[0]
    n_rows = direct_ref.shape[0]
    model, ff = wg_ref.shape
    sums = (ga, ua, da, gb, ub, db)
    for ref, start in zip(sums, (ga_in, ua_in, da_in, gb_in, ub_in, db_in)):
        ref[...] = start[...]
    width = far_lo_ref.shape[1] // 3
    at = block_rows(tp, 2, width)
    wg, wu, wd = wg_ref[at, :], wu_ref[at, :], wd_ref[:, at]
    gather_products(sums, 0, far_lo_ref, wg, wu, wd, False)
    gather_products(sums, n_rows // 2, far_hi_ref, wg, wu, wd, False)
    at = slice(4 * width, model)
    gather_products(sums, 0, direct_ref, wg_ref[at, :], wu_ref[at, :], wd_ref[:, at], False)

    def local(g, u, d):
        sigma = 1.0 / (1.0 + jnp.exp(-g))
        silu = g * sigma
        return d * u * sigma * (1.0 + g * (1.0 - sigma)), d * silu, silu * u

    p, q, r = local(ga[...], ua[...], da[...])
    da_out[:, 0:ff] = p.astype(BF)
    da_out[:, ff : 2 * ff] = q.astype(BF)
    da_out[:, 2 * ff : 3 * ff] = r.astype(BF)
    keep = lax.rem(lax.broadcasted_iota(jnp.int32, (n_rows, ff), 0), 8) < 4
    p, q, r = local(gb[...], ub[...], pltpu.roll(db[...], n_rows - 4, 0))
    p, q, r = (jnp.where(keep, v, 0.0) for v in (p, q, r))
    db_out[:, 0:ff] = p.astype(BF)
    db_out[:, ff : 2 * ff] = q.astype(BF)
    db_out[:, 2 * ff : 3 * ff] = pltpu.roll(r, 4, 0).astype(BF)
    db_out[:, 3 * ff : 4 * ff] = pltpu.roll(p, 4, 0).astype(BF)
    db_out[:, 4 * ff :] = pltpu.roll(q, 4, 0).astype(BF)
    share = model // 4
    at = block_rows(tp, 2, share)
    high_p, high_q = db_out[:, 3 * ff : 4 * ff], db_out[:, 4 * ff :]
    write_rows(
        (far_lo_out, far_hi_out),
        *partial_rows(da_out, db_out, high_p, high_q, wg_ref[at, :], wu_ref[at, :]),
    )


def near_kernel(
    tp_ref, da, db, wg_ref, wu_ref, up_lo_out, up_hi_out, down_lo_out, down_hi_out, own_out
):
    tp = tp_ref[0]
    model, ff = wg_ref.shape
    high_p, high_q = db[:, 3 * ff : 4 * ff], db[:, 4 * ff :]
    for by, refs in ((1, (up_lo_out, up_hi_out)), (3, (down_lo_out, down_hi_out)), (0, (own_out,))):
        at = block_rows(tp, by, model // 4)
        write_rows(refs, *partial_rows(da, db, high_p, high_q, wg_ref[at, :], wu_ref[at, :]))


def weights_kernel(
    tp_ref, own_ref, prev_ref, next_ref, far_lo_ref, far_hi_ref, direct_ref, da_ref, db_ref,
    gg_ref, gu_ref, gd_ref,
):
    tp = tp_ref[0]
    width = own_ref.shape[1] // 3
    half = own_ref.shape[0] // 2
    ff, model = gd_ref.shape

    def sums(x_ref, lo):
        n, wide = x_ref.shape[0], x_ref.shape[1] // 3
        da, db = da_ref[lo : lo + n, :], db_ref[lo : lo + n, :]
        h, s, m = x_ref[:, 0:wide], x_ref[:, wide : 2 * wide], x_ref[:, 2 * wide :]
        both = tn(h, da[:, 0 : 2 * ff]) + tn(m, db[:, 0 : 2 * ff])
        down = tn(da[:, 2 * ff : 3 * ff], s) + tn(db[:, 2 * ff : 3 * ff], m)
        return both, down

    def put(at, both, down):
        gg_ref[at, :] = both[:, 0:ff].astype(BF)
        gu_ref[at, :] = both[:, ff:].astype(BF)
        gd_ref[:, at] = down.astype(BF)

    put(block_rows(tp, 0, width), *sums(own_ref, 0))
    put(block_rows(tp, 3, width), *sums(prev_ref, 0))
    put(block_rows(tp, 1, width), *sums(next_ref, 0))
    both, down = sums(far_lo_ref, 0)
    both_hi, down_hi = sums(far_hi_ref, half)
    put(block_rows(tp, 2, width), both + both_hi, down + down_hi)
    put(slice(4 * width, model), *sums(direct_ref, 0))


def mixer_kernel(
    where_ref, res_ref, wo_own, wo_prev, wo_next, wo_far, y_own, y_prev, y_next, y_far,
    dy_own, dy_prev, dy_next, dy_far, mine_ref, other_ref,
):
    tp, core = where_ref[0], where_ref[1]
    res = res_ref[...]
    width = res.shape[1]
    for w_ref, y_ref, dy_ref, by in (
        (wo_own, y_own, dy_own, 0),
        (wo_prev, y_prev, dy_prev, 3),
        (wo_next, y_next, dy_next, 1),
        (wo_far, y_far, dy_far, 2),
    ):
        dy_ref[...] = nn(res, w_ref[...]).astype(dy_ref.dtype)
        grad = tn(res, y_ref[...]).astype(BF).reshape(width // 64, 2, 32, y_ref.shape[1])
        low, high = grad[:, 0], grad[:, 1]
        shape = (width // 2, y_ref.shape[1])
        to = block_rows(tp, by, width // 2)
        first = core == 0
        mine_ref[to, :] = jnp.where(first, low, high).reshape(shape)
        other_ref[to, :] = jnp.where(first, high, low).reshape(shape)


def from_behind(x, by):
    n = lax.axis_size(SP)
    return lax.ppermute(x, SP, [(i, i + by) for i in range(n) if 0 <= i + by < n])


def ring(x):
    half = x.shape[0] // 2
    prev = shifted(x, "y", 1)
    after = shifted(x, "y", -1)
    return prev, after, shifted(prev[:half], "y", 1), shifted(after[half:], "y", -1)


def per_device(
    hidden_in, cotangent, routes, routing_weights, w_gate, w_up, w_down, b_gate, c_gate, x_in, taps, w_out
):
    tok_rows, model_width = hidden_in.shape
    share = model_width // 4
    chan = w_out.shape[1]
    y_at = lax.axis_index("y").astype(jnp.int32)
    tp = y_at.reshape(1)
    where = jnp.stack([y_at, lax.axis_index("c").astype(jnp.int32)])
    wg, wu, wd = w_gate[0], w_up[0], w_down[0]
    ff = wg.shape[1]

    sent, sent_direct, rows = route(tp, routes.T, routing_weights.T, hidden_in, cotangent)
    to_experts = lambda v: lax.all_to_all(
        v.reshape(64, MAIN, v.shape[1]), SP, split_axis=0, concat_axis=0, tiled=True
    ).reshape(v.shape)
    tail = slice(tok_rows - 2, tok_rows)
    earlier = from_behind(c_gate[tail].astype(F32) * x_in[tail].astype(F32), 1)
    sent, earlier = lax.optimization_barrier((sent, earlier))
    own = to_experts(sent)

    taps_f = taps.astype(F32)
    gated = c_gate.astype(F32) * x_in.astype(F32)
    padded = jnp.concatenate([earlier, gated], axis=0)
    conv = (
        taps_f[0] * padded[0:tok_rows]
        + taps_f[1] * padded[1 : tok_rows + 1]
        + taps_f[2] * padded[2 : tok_rows + 2]
    )
    y_short = (b_gate.astype(F32) * conv).astype(BF)
    y_blocks = (y_short, shifted(y_short, "y", 1), shifted(y_short, "y", -1), shifted(y_short, "y", 2))
    part = lambda by: lax.dynamic_slice_in_dim(w_out, lax.rem(y_at + by, 4) * share, share, 0)
    wo_blocks = (part(0), shifted(part(1), "y", 1), shifted(part(3), "y", -1), shifted(part(2), "y", 2))
    own, sent_direct, conv, *held = lax.optimization_barrier(
        (own, sent_direct, conv, *y_blocks, *wo_blocks)
    )
    y_blocks, wo_blocks = held[:4], held[4:]

    prev, after, far_lo, far_hi = ring(own)
    direct = to_experts(sent_direct)

    n_rows, half = own.shape[0], own.shape[0] // 2
    out_width = share + share // 2
    sums = local_call(early_kernel, tp, (own, prev, after, wg, wu, wd), [((n_rows, ff), F32)] * 6)
    da, db, f_lo, f_hi = local_call(
        late_kernel, tp, (*sums, far_lo, far_hi, direct, wg, wu, wd),
        [((n_rows, 3 * ff), BF), ((n_rows, 5 * ff), BF), ((half, out_width), BF), ((half, out_width), BF)],
        [pltpu.VMEM((n_rows, ff), F32)] * 6,
    )
    u_lo, u_hi, d_lo, d_hi, o = local_call(
        near_kernel, tp, (da, db, wg, wu),
        [((half, out_width), BF)] * 4 + [((n_rows, out_width), BF)],
    )

    from_prev = shifted(f_lo, "y", 1)
    from_next = shifted(f_hi, "y", -1)
    prev_hi = shifted(u_hi, "y", 1)
    next_lo = shifted(d_lo, "y", -1)
    added = lambda a, b: (a.astype(F32) + b.astype(F32)).astype(BF)
    prev_lo = shifted(added(u_lo, from_prev), "y", 1)
    next_hi = shifted(added(d_hi, from_next), "y", -1)
    got_prev = jnp.concatenate([prev_lo, prev_hi], axis=0).astype(F32)
    got_next = jnp.concatenate([next_lo, next_hi], axis=0).astype(F32)
    total = (o.astype(F32) + got_prev + got_next).astype(BF)
    back = to_experts(total)
    gg, gu, gd = local_call(
        weights_kernel, tp, (own, prev, after, far_lo, far_hi, direct, da, db),
        [((model_width, ff), BF), ((model_width, ff), BF), ((ff, model_width), BF)],
    )
    back, gg, gu, gd = lax.optimization_barrier((back, gg, gu, gd))

    residual_grad = combine(tp, rows, back, cotangent)
    dy, dy_prev, dy_next, dy_far, mine, other = local_call(
        mixer_kernel, where, (residual_grad, *wo_blocks, *y_blocks),
        [((tok_rows, chan), F32)] + [((tok_rows, chan), BF)] * 3 + [((2 * share, chan), BF)] * 2,
    )
    chip = added(mine, shifted(other, "c", 1)).reshape(32, 32, chan)
    d_y = (
        dy
        + shifted(dy_prev, "y", -1).astype(F32)
        + shifted(dy_next, "y", 1).astype(F32)
        + shifted(dy_far, "y", 2).astype(F32)
    )
    grad_b = (d_y * conv).astype(BF)
    d_conv = b_gate.astype(F32) * d_y
    following = from_behind(d_conv[0:2], -1)
    later = jnp.concatenate([d_conv, following], axis=0)
    d_v = (
        taps_f[2] * later[0:tok_rows]
        + taps_f[1] * later[1 : tok_rows + 1]
        + taps_f[0] * later[2 : tok_rows + 2]
    )
    grad_c = (d_v * x_in.astype(F32)).astype(BF)
    grad_x = (d_v * c_gate.astype(F32)).astype(BF)

    parts = lax.all_to_all(chip, ("z", "x"), split_axis=0, concat_axis=0, tiled=True)
    piece = jnp.sum(parts.astype(F32), axis=0)
    at = lambda z, x, c, y: ((z * 4 + x) * 2 + c) * 4 + y
    pairs = [
        (at(z, x, c, y), at(2 * y + z % 2, x, c, z // 2))
        for z in range(8) for x in range(4) for c in range(2) for y in range(4)
    ]
    out_proj_grad = lax.ppermute(piece, ("z", "x", "c", "y"), pairs)

    return (gg[None], gu[None], gd[None], out_proj_grad, residual_grad, grad_b, grad_c, grad_x)


def solution(mesh):
    fine = Mesh(mesh.devices.reshape(8, 4, 2, 4), ("z", "x", "c", "y"))
    rows = P(SP, None)
    both = P(SP, "y")
    return jax.shard_map(
        per_device,
        mesh=fine,
        in_specs=(
            rows, rows, rows, rows,
            P(SP, None, "y"), P(SP, None, "y"), P(SP, "y", None),
            both, both, both, P(None, "y"), P(None, "y"),
        ),
        out_specs=(P(SP, None, "y"), P(SP, None, "y"), P(SP, "y", None), both, both, both, both, both),
        check_vma=False,
    )
```

```python
import jax
import jax.numpy as jnp
from jax import lax
from jax.experimental import pallas as pl
from jax.experimental.pallas import tpu as pltpu
from jax.sharding import Mesh, PartitionSpec as P

BF = jnp.bfloat16
F32 = jnp.float32
SP = ("z", "x", "c")
MAIN = 8
VMEM_LIMIT = 56 * 1024 * 1024
SMALL_LIMIT = 20 * 1024 * 1024


def dot(a, b, contract):
    return lax.dot_general(a, b, ((contract[0], contract[1]), ((), ())), preferred_element_type=F32)


def nn(a, b):
    return dot(a, b, ((1,), (0,)))


def nt(a, b):
    return dot(a, b, ((1,), (1,)))


def tn(a, b):
    return dot(a, b, ((0,), (0,)))


def shifted(x, axis, by):
    n = lax.axis_size(axis)
    return lax.ppermute(x, axis, [(i, (i + by) % n) for i in range(n)])


def selection(row, base=0):
    n_rows = 64 * MAIN
    at = lax.broadcasted_iota(jnp.int32, (n_rows, row.shape[1]), 0)
    return at == (row + base)


def route_kernel(tp_ref, ids_ref, w_ref, h_ref, c_ref, hd_ref, cd_ref, out_ref, direct_ref, rows_ref):
    tokens = ids_ref.shape[1]
    expert = lax.broadcasted_iota(jnp.int32, (64, tokens), 0)
    upper = (
        lax.broadcasted_iota(jnp.int32, (tokens, tokens), 0)
        < lax.broadcasted_iota(jnp.int32, (tokens, tokens), 1)
    ).astype(F32).astype(BF)
    ids0, ids1 = ids_ref[0:1, :], ids_ref[1:2, :]
    hot0 = (expert == ids0).astype(F32)
    hot1 = (expert == ids1).astype(F32)
    before0 = nn(hot0.astype(BF), upper)
    before1 = nn(hot1.astype(BF), upper) + jnp.sum(hot0, axis=1, keepdims=True)
    pos0 = jnp.sum(hot0 * before0, axis=0, keepdims=True).astype(jnp.int32)
    pos1 = jnp.sum(hot1 * before1, axis=0, keepdims=True).astype(jnp.int32)
    w0, w1 = w_ref[0:1, :], w_ref[1:2, :]
    none = jnp.full_like(ids0, -64)
    a0 = jnp.where(pos0 < MAIN, ids0 * MAIN + pos0, none)
    a1 = jnp.where(pos1 < MAIN, ids1 * MAIN + pos1, none)
    b0 = jnp.where((pos0 >= MAIN) & (pos0 < MAIN + 4), ids0 * MAIN + pos0 - MAIN, none)
    b1 = jnp.where((pos1 >= MAIN) & (pos1 < MAIN + 4), ids1 * MAIN + pos1 - MAIN, none)
    rows_ref[0:1, :] = a0
    rows_ref[1:2, :] = a1
    rows_ref[2:3, :] = b0
    rows_ref[3:4, :] = b1

    def picked(r0, r1, base):
        s0, s1 = selection(r0, base), selection(r1, base)
        weight = jnp.sum(jnp.where(s0, w0, 0.0) + jnp.where(s1, w1, 0.0), axis=1, keepdims=True)
        return (s0 | s1).astype(F32).astype(BF), weight

    sel, weight = picked(a0, a1, 0)
    sel_h, _ = picked(b0, b1, 0)
    sel_s, weight_s = picked(b0, b1, 4)
    for h_in, c_in, to in ((h_ref, c_ref, out_ref), (hd_ref, cd_ref, direct_ref)):
        h, c = h_in[...], c_in[...]
        width = h.shape[1]
        to[:, 0:width] = nn(sel, h).astype(BF)
        to[:, width : 2 * width] = (nn(sel, c) * weight).astype(BF)
        to[:, 2 * width :] = (nn(sel_h, h) + nn(sel_s, c) * weight_s).astype(BF)


def route(tp, ids, weights, hidden_in, cotangent):
    tokens, width = hidden_in.shape
    direct = width // 4
    ring = (width - direct) // 4
    share = pl.BlockSpec((tokens, ring), lambda i, t: (0, t[0]))
    last = pl.BlockSpec((tokens, direct), lambda i, t: (0, 3))
    whole = lambda shape: pl.BlockSpec(shape, lambda i, t: (0, 0))
    return pl.pallas_call(
        route_kernel,
        grid_spec=pltpu.PrefetchScalarGridSpec(
            num_scalar_prefetch=1,
            grid=(1,),
            in_specs=[whole(ids.shape), whole(weights.shape), share, share, last, last],
            out_specs=[whole((64 * MAIN, 3 * ring)), whole((64 * MAIN, 3 * direct)), whole((4, tokens))],
        ),
        out_shape=[
            jax.ShapeDtypeStruct((64 * MAIN, 3 * ring), BF),
            jax.ShapeDtypeStruct((64 * MAIN, 3 * direct), BF),
            jax.ShapeDtypeStruct((4, tokens), jnp.int32),
        ],
        compiler_params=pltpu.CompilerParams(vmem_limit_bytes=VMEM_LIMIT),
        name="route",
    )(tp, ids, weights, hidden_in, cotangent, hidden_in, cotangent)


def combine_kernel(
    tp_ref, rows_ref, back_ref, c_ref, wo_own, wo_prev, wo_next, wo_far,
    out_ref, dy_own, dy_prev, dy_next, dy_far,
):
    width = c_ref.shape[1]
    a0, a1, b0, b1 = (rows_ref[k : k + 1, :] for k in range(4))

    def sel(r0, r1, base):
        return (selection(r0, base) | selection(r1, base)).astype(F32).astype(BF)

    main = tn(sel(a0, a1, 0), back_ref[:, 0:width])
    rest = back_ref[:, width:]
    low = tn(sel(b0, b1, 0), rest)
    high = tn(sel(b0, b1, 4), rest)
    half = width // 2
    out_ref[:, 0:half] = (c_ref[:, 0:half].astype(F32) + (main[:, 0:half] + low)).astype(BF)
    out_ref[:, half:] = (c_ref[:, half:].astype(F32) + (main[:, half:] + high)).astype(BF)
    res = out_ref[...]
    for w_ref, dy in ((wo_own, dy_own), (wo_prev, dy_prev), (wo_next, dy_next), (wo_far, dy_far)):
        dy[...] = nn(res, w_ref[...]).astype(dy.dtype)


def combine(tp, rows, back, cotangent, wo_blocks):
    tokens, width = cotangent.shape[0], cotangent.shape[1] // 4
    chan = wo_blocks[0].shape[1]
    whole = lambda shape: pl.BlockSpec(shape, lambda i, t: (0, 0))
    return pl.pallas_call(
        combine_kernel,
        grid_spec=pltpu.PrefetchScalarGridSpec(
            num_scalar_prefetch=1,
            grid=(1,),
            in_specs=[
                whole(rows.shape),
                whole(back.shape),
                pl.BlockSpec((tokens, width), lambda i, t: (0, t[0])),
            ]
            + [whole((width, chan))] * 4,
            out_specs=[whole((tokens, width))] + [whole((tokens, chan))] * 4,
        ),
        out_shape=[jax.ShapeDtypeStruct((tokens, width), BF), jax.ShapeDtypeStruct((tokens, chan), F32)]
        + [jax.ShapeDtypeStruct((tokens, chan), BF)] * 3,
        compiler_params=pltpu.CompilerParams(vmem_limit_bytes=SMALL_LIMIT),
        name="combine",
    )(tp, rows, back, in_hbm(cotangent), *map(in_hbm, wo_blocks))


def block_at(tp, by):
    return lax.rem(tp + by, 4)


def vmem_specs(n):
    return [pl.BlockSpec(memory_space=pltpu.VMEM) for _ in range(n)]


def in_hbm(x):
    return pltpu.with_memory_space_constraint(x, pltpu.HBM)


def local_call(kernel, scalars, arrays, outs, limit=VMEM_LIMIT):
    return pl.pallas_call(
        kernel,
        in_specs=[pl.BlockSpec(memory_space=pltpu.SMEM)] + vmem_specs(len(arrays)),
        out_specs=vmem_specs(len(outs)),
        out_shape=[jax.ShapeDtypeStruct(shape, dtype) for shape, dtype in outs],
        compiler_params=pltpu.CompilerParams(vmem_limit_bytes=limit),
    )(scalars, *arrays)


def block_rows(tp, by, width):
    return pl.ds(pl.multiple_of(block_at(tp, by) * width, width), width)


def gather_products(sums, lo, x_ref, wg, wu, wd, first):
    ga, ua, da, gb, ub, db = sums
    width = x_ref.shape[1] // 3
    to = slice(lo, lo + x_ref.shape[0])
    h, s, m = x_ref[:, 0:width], x_ref[:, width : 2 * width], x_ref[:, 2 * width :]

    def add(ref, x):
        ref[to, :] = x if first else ref[to, :] + x

    add(ga, nn(h, wg))
    add(ua, nn(h, wu))
    add(da, nt(s, wd))
    add(gb, nn(m, wg))
    add(ub, nn(m, wu))
    add(db, nt(m, wd))


def early_kernel(tp_ref, own_ref, prev_ref, next_ref, wg_ref, wu_ref, wd_ref, *sums):
    tp = tp_ref[0]
    width = own_ref.shape[1] // 3
    for ref, by in ((own_ref, 0), (prev_ref, 3), (next_ref, 1)):
        at = block_rows(tp, by, width)
        gather_products(sums, 0, ref, wg_ref[at, :], wu_ref[at, :], wd_ref[:, at], by == 0)


def partial_rows(da, db, high_p, high_q, wg, wu):
    ff = wg.shape[1]
    cut = wg.shape[0] // 2
    main = nt(da[:, 0:ff], wg) + nt(da[:, ff : 2 * ff], wu)
    rest = nt(db[:, 0:ff], wg[0:cut]) + nt(db[:, ff : 2 * ff], wu[0:cut])
    rest = rest + nt(high_p, wg[cut:]) + nt(high_q, wu[cut:])
    return main.astype(BF), rest.astype(BF)


def write_rows(refs, main, rest):
    at = 0
    for ref in refs:
        n, width = ref.shape[0], main.shape[1]
        ref[:, 0:width] = main[at : at + n]
        ref[:, width:] = rest[at : at + n]
        at += n


def late_kernel(
    tp_ref, ga_in, ua_in, da_in, gb_in, ub_in, db_in, far_lo_in, far_hi_in, direct_in,
    wg_in, wu_in, wd_in, da_out, db_out, far_lo_out, far_hi_out,
    ga, ua, da, gb, ub, db, ga_s, ua_s, da_s, gb_s, ub_s, db_s,
    far, wg_d, wu_d, wd_d, wg_f, wu_f, wd_f, wg_o, wu_o, sems,
):
    tp = tp_ref[0]
    n_rows, ff = ga.shape
    half = n_rows // 2
    width, tail = wg_f.shape[0], wg_d.shape[0]
    last = slice(4 * width, 4 * width + tail)
    opposite = block_rows(tp, 2, width)
    share = block_rows(tp, 2, wg_o.shape[0])
    moves = [
        (wg_in.at[last, :], wg_d), (wu_in.at[last, :], wu_d), (wd_in.at[:, last], wd_d),
        (far_lo_in, far.at[0:half, :]), (far_hi_in, far.at[half:n_rows, :]),
        (wg_in.at[opposite, :], wg_f), (wu_in.at[opposite, :], wu_f), (wd_in.at[:, opposite], wd_f),
        (ga_in, ga_s), (ua_in, ua_s), (da_in, da_s), (gb_in, gb_s), (ub_in, ub_s), (db_in, db_s),
        (wg_in.at[share, :], wg_o), (wu_in.at[share, :], wu_o),
    ]
    copies = [pltpu.make_async_copy(src, dst, sems.at[k]) for k, (src, dst) in enumerate(moves)]
    for copy in copies:
        copy.start()
    sums = (ga, ua, da, gb, ub, db)
    for copy in copies[0:3]:
        copy.wait()
    gather_products(sums, 0, direct_in, wg_d[...], wu_d[...], wd_d[...], True)
    for copy in copies[3:8]:
        copy.wait()
    gather_products(sums, 0, far, wg_f[...], wu_f[...], wd_f[...], False)
    for copy in copies[8:16]:
        copy.wait()

    def local(g, u, d):
        sigma = 1.0 / (1.0 + jnp.exp(-g))
        silu = g * sigma
        return d * u * sigma * (1.0 + g * (1.0 - sigma)), d * silu, silu * u

    p, q, r = local(ga[...] + ga_s[...], ua[...] + ua_s[...], da[...] + da_s[...])
    da_out[:, 0:ff] = p.astype(BF)
    da_out[:, ff : 2 * ff] = q.astype(BF)
    da_out[:, 2 * ff : 3 * ff] = r.astype(BF)
    keep = lax.rem(lax.broadcasted_iota(jnp.int32, (n_rows, ff), 0), 8) < 4
    p, q, r = local(gb[...] + gb_s[...], ub[...] + ub_s[...], pltpu.roll(db[...] + db_s[...], n_rows - 4, 0))
    p, q, r = (jnp.where(keep, v, 0.0) for v in (p, q, r))
    db_out[:, 0:ff] = p.astype(BF)
    db_out[:, ff : 2 * ff] = q.astype(BF)
    db_out[:, 2 * ff : 3 * ff] = pltpu.roll(r, 4, 0).astype(BF)
    db_out[:, 3 * ff : 4 * ff] = pltpu.roll(p, 4, 0).astype(BF)
    db_out[:, 4 * ff :] = pltpu.roll(q, 4, 0).astype(BF)
    high_p, high_q = db_out[:, 3 * ff : 4 * ff], db_out[:, 4 * ff :]
    write_rows((far_lo_out, far_hi_out), *partial_rows(da_out, db_out, high_p, high_q, wg_o[...], wu_o[...]))


def late(tp, sums, far_lo, far_hi, direct, wg, wu, wd):
    n_rows, ff = sums[0].shape
    model = wg.shape[0]
    width, tail = far_lo.shape[1] // 3, direct.shape[1] // 3
    share = model // 4
    piece = jax.ShapeDtypeStruct((n_rows // 2, share + share // 2), BF)
    vmem = pltpu.VMEM
    return pl.pallas_call(
        late_kernel,
        in_specs=[pl.BlockSpec(memory_space=pltpu.SMEM)]
        + [pl.BlockSpec(memory_space=pltpu.HBM)] * 8
        + vmem_specs(1)
        + [pl.BlockSpec(memory_space=pltpu.HBM)] * 3,
        out_specs=vmem_specs(4),
        out_shape=[
            jax.ShapeDtypeStruct((n_rows, 3 * ff), BF), jax.ShapeDtypeStruct((n_rows, 5 * ff), BF), piece, piece,
        ],
        scratch_shapes=[vmem((n_rows, ff), F32)] * 12
        + [vmem((n_rows, 3 * width), BF)]
        + [vmem((tail, ff), BF), vmem((tail, ff), BF), vmem((ff, tail), BF)]
        + [vmem((width, ff), BF), vmem((width, ff), BF), vmem((ff, width), BF)]
        + [vmem((share, ff), BF), vmem((share, ff), BF), pltpu.SemaphoreType.DMA((16,))],
        compiler_params=pltpu.CompilerParams(vmem_limit_bytes=SMALL_LIMIT),
        name="late",
    )(tp, *map(in_hbm, sums), far_lo, far_hi, direct, in_hbm(wg), in_hbm(wu), in_hbm(wd))


def near_kernel(
    tp_ref, da, db, wg_ref, wu_ref, up_lo_out, up_hi_out, down_lo_out, down_hi_out, own_out
):
    tp = tp_ref[0]
    model, ff = wg_ref.shape
    high_p, high_q = db[:, 3 * ff : 4 * ff], db[:, 4 * ff :]
    for by, refs in ((1, (up_lo_out, up_hi_out)), (3, (down_lo_out, down_hi_out)), (0, (own_out,))):
        at = block_rows(tp, by, model // 4)
        write_rows(refs, *partial_rows(da, db, high_p, high_q, wg_ref[at, :], wu_ref[at, :]))


def weights_kernel(
    tp_ref, own_ref, prev_ref, next_ref, far_lo_ref, far_hi_ref, direct_ref, da_ref, db_ref,
    gg_ref, gu_ref, gd_ref,
):
    tp = tp_ref[0]
    width = own_ref.shape[1] // 3
    half = own_ref.shape[0] // 2
    ff, model = gd_ref.shape

    def sums(x_ref, lo):
        n, wide = x_ref.shape[0], x_ref.shape[1] // 3
        da, db = da_ref[lo : lo + n, :], db_ref[lo : lo + n, :]
        h, s, m = x_ref[:, 0:wide], x_ref[:, wide : 2 * wide], x_ref[:, 2 * wide :]
        both = tn(h, da[:, 0 : 2 * ff]) + tn(m, db[:, 0 : 2 * ff])
        down = tn(da[:, 2 * ff : 3 * ff], s) + tn(db[:, 2 * ff : 3 * ff], m)
        return both, down

    def put(at, both, down):
        gg_ref[at, :] = both[:, 0:ff].astype(BF)
        gu_ref[at, :] = both[:, ff:].astype(BF)
        gd_ref[:, at] = down.astype(BF)

    put(block_rows(tp, 0, width), *sums(own_ref, 0))
    put(block_rows(tp, 3, width), *sums(prev_ref, 0))
    put(block_rows(tp, 1, width), *sums(next_ref, 0))
    both, down = sums(far_lo_ref, 0)
    both_hi, down_hi = sums(far_hi_ref, half)
    put(block_rows(tp, 2, width), both + both_hi, down + down_hi)
    put(slice(4 * width, model), *sums(direct_ref, 0))


def mixer_kernel(where_ref, res_ref, res_o_ref, y_ref, y_o_ref, out_ref):
    tp, core = lax.rem(where_ref[0], 4), lax.div(where_ref[0], 4)
    width = res_ref.shape[1]
    chan = out_ref.shape[1]
    for k, by in enumerate((0, 3, 1, 2)):
        at = slice(k * chan, (k + 1) * chan)
        grad = tn(res_ref[...], y_ref[:, at]) + tn(res_o_ref[...], y_o_ref[:, at])
        grad = grad.reshape(width // 64, 2, 32, chan)
        mine = jnp.where(core == 0, grad[:, 0], grad[:, 1]).reshape(width // 2, chan)
        out_ref[block_rows(tp, by, width // 2), :] = mine.astype(BF)


def from_behind(x, by):
    n = lax.axis_size(SP)
    return lax.ppermute(x, SP, [(i, i + by) for i in range(n) if 0 <= i + by < n])


def ring(x):
    half = x.shape[0] // 2
    prev = shifted(x, "y", 1)
    after = shifted(x, "y", -1)
    return prev, after, shifted(prev[:half], "y", 1), shifted(after[half:], "y", -1)


def per_device(
    hidden_in, cotangent, routes, routing_weights, w_gate, w_up, w_down, b_gate, c_gate, x_in, taps, w_out
):
    tok_rows, model_width = hidden_in.shape
    share = model_width // 4
    chan = w_out.shape[1]
    y_at = lax.axis_index("y").astype(jnp.int32)
    tp = y_at.reshape(1)
    where = (y_at + 4 * lax.axis_index("c").astype(jnp.int32)).reshape(1)
    wg, wu, wd = w_gate[0], w_up[0], w_down[0]
    ff = wg.shape[1]

    sent, sent_direct, rows = route(tp, routes.T, routing_weights.T, hidden_in, cotangent)
    to_experts = lambda v: lax.all_to_all(
        v.reshape(64, MAIN, v.shape[1]), SP, split_axis=0, concat_axis=0, tiled=True
    ).reshape(v.shape)
    tail = slice(tok_rows - 2, tok_rows)
    earlier = from_behind(c_gate[tail].astype(F32) * x_in[tail].astype(F32), 1)
    sent, earlier = lax.optimization_barrier((sent, earlier))
    own = to_experts(sent)

    taps_f = taps.astype(F32)
    gated = c_gate.astype(F32) * x_in.astype(F32)
    padded = jnp.concatenate([earlier, gated], axis=0)
    conv = (
        taps_f[0] * padded[0:tok_rows]
        + taps_f[1] * padded[1 : tok_rows + 1]
        + taps_f[2] * padded[2 : tok_rows + 2]
    )
    y_short = (b_gate.astype(F32) * conv).astype(BF)
    y_all = jnp.concatenate(
        (y_short, shifted(y_short, "y", 1), shifted(y_short, "y", -1), shifted(y_short, "y", 2)), axis=1
    )
    part = lambda by: lax.dynamic_slice_in_dim(w_out, lax.rem(y_at + by, 4) * share, share, 0)
    wo_blocks = (part(0), shifted(part(1), "y", 1), shifted(part(3), "y", -1), shifted(part(2), "y", 2))
    own, sent_direct, conv, y_all, *wo_blocks = lax.optimization_barrier(
        (own, sent_direct, conv, y_all, *wo_blocks)
    )
    y_other = shifted(y_all, "c", 1)

    prev, after, far_lo, far_hi = ring(own)
    far_lo, far_hi = in_hbm(far_lo), in_hbm(far_hi)
    direct = to_experts(sent_direct)

    n_rows, half = own.shape[0], own.shape[0] // 2
    out_width = share + share // 2
    sums = local_call(early_kernel, tp, (own, prev, after, wg, wu, wd), [((n_rows, ff), F32)] * 6)
    da, db, f_lo, f_hi = late(tp, sums, far_lo, far_hi, direct, wg, wu, wd)
    u_lo, u_hi, d_lo, d_hi, o = local_call(
        near_kernel, tp, (da, db, in_hbm(wg), in_hbm(wu)),
        [((half, out_width), BF)] * 4 + [((n_rows, out_width), BF)], SMALL_LIMIT,
    )

    from_prev = shifted(f_lo, "y", 1)
    from_next = shifted(f_hi, "y", -1)
    prev_hi = shifted(u_hi, "y", 1)
    next_lo = shifted(d_lo, "y", -1)
    added = lambda a, b: (a.astype(F32) + b.astype(F32)).astype(BF)
    prev_lo = shifted(added(u_lo, from_prev), "y", 1)
    next_hi = shifted(added(d_hi, from_next), "y", -1)
    got_prev = jnp.concatenate([prev_lo, prev_hi], axis=0).astype(F32)
    got_next = jnp.concatenate([next_lo, next_hi], axis=0).astype(F32)
    total = (o.astype(F32) + got_prev + got_next).astype(BF)
    back = to_experts(total)
    gg, gu, gd = local_call(
        weights_kernel, tp, (own, prev, after, far_lo, far_hi, direct, da, db),
        [((model_width, ff), BF), ((model_width, ff), BF), ((ff, model_width), BF)],
    )
    back, gg, gu, gd, y_other = lax.optimization_barrier((back, gg, gu, gd, y_other))

    residual_grad, dy, dy_prev, dy_next, dy_far = combine(tp, rows, back, cotangent, wo_blocks)
    res_other = shifted(residual_grad, "c", 1)
    (chip,) = local_call(
        mixer_kernel, where, (in_hbm(residual_grad), res_other, in_hbm(y_all), in_hbm(y_other)),
        [((2 * share, chan), BF)], SMALL_LIMIT,
    )
    d_y = (
        dy
        + shifted(dy_prev, "y", -1).astype(F32)
        + shifted(dy_next, "y", 1).astype(F32)
        + shifted(dy_far, "y", 2).astype(F32)
    )
    grad_b = (d_y * conv).astype(BF)
    d_conv = b_gate.astype(F32) * d_y
    following = from_behind(d_conv[0:2], -1)
    later = jnp.concatenate([d_conv, following], axis=0)
    d_v = (
        taps_f[2] * later[0:tok_rows]
        + taps_f[1] * later[1 : tok_rows + 1]
        + taps_f[0] * later[2 : tok_rows + 2]
    )
    grad_c = (d_v * x_in.astype(F32)).astype(BF)
    grad_x = (d_v * c_gate.astype(F32)).astype(BF)

    parts = lax.all_to_all(chip.reshape(32, 32, chan), ("z", "x"), split_axis=0, concat_axis=0, tiled=True)
    piece = jnp.sum(parts.astype(F32), axis=0)
    at = lambda z, x, c, y: ((z * 4 + x) * 2 + c) * 4 + y
    pairs = [
        (at(z, x, c, y), at(2 * y + z % 2, x, c, z // 2))
        for z in range(8) for x in range(4) for c in range(2) for y in range(4)
    ]
    out_proj_grad = lax.ppermute(piece, ("z", "x", "c", "y"), pairs)

    return (gg[None], gu[None], gd[None], out_proj_grad, residual_grad, grad_b, grad_c, grad_x)


def solution(mesh):
    fine = Mesh(mesh.devices.reshape(8, 4, 2, 4), ("z", "x", "c", "y"))
    rows = P(SP, None)
    both = P(SP, "y")
    return jax.shard_map(
        per_device,
        mesh=fine,
        in_specs=(
            rows, rows, rows, rows,
            P(SP, None, "y"), P(SP, None, "y"), P(SP, "y", None),
            both, both, both, P(None, "y"), P(None, "y"),
        ),
        out_specs=(P(SP, None, "y"), P(SP, None, "y"), P(SP, "y", None), both, both, both, both, both),
        check_vma=False,
    )
```

```python
import jax
import jax.numpy as jnp
from jax import lax
from jax.experimental import pallas as pl
from jax.experimental.pallas import tpu as pltpu
from jax.sharding import Mesh, PartitionSpec as P

BF = jnp.bfloat16
F32 = jnp.float32
SP = ("z", "x", "c")
MAIN = 8
VMEM_LIMIT = 56 * 1024 * 1024
SMALL_LIMIT = 20 * 1024 * 1024


def dot(a, b, contract):
    return lax.dot_general(a, b, ((contract[0], contract[1]), ((), ())), preferred_element_type=F32)


def nn(a, b):
    return dot(a, b, ((1,), (0,)))


def nt(a, b):
    return dot(a, b, ((1,), (1,)))


def tn(a, b):
    return dot(a, b, ((0,), (0,)))


def shifted(x, axis, by):
    n = lax.axis_size(axis)
    return lax.ppermute(x, axis, [(i, (i + by) % n) for i in range(n)])


def selection(row, base=0):
    n_rows = 64 * MAIN
    at = lax.broadcasted_iota(jnp.int32, (n_rows, row.shape[1]), 0)
    return at == (row + base)


def route_kernel(tp_ref, ids_ref, w_ref, h_ref, c_ref, hd_ref, cd_ref, out_ref, direct_ref, rows_ref):
    tokens = ids_ref.shape[1]
    expert = lax.broadcasted_iota(jnp.int32, (64, tokens), 0)
    upper = (
        lax.broadcasted_iota(jnp.int32, (tokens, tokens), 0)
        < lax.broadcasted_iota(jnp.int32, (tokens, tokens), 1)
    ).astype(F32).astype(BF)
    ids0, ids1 = ids_ref[0:1, :], ids_ref[1:2, :]
    hot0 = (expert == ids0).astype(F32)
    hot1 = (expert == ids1).astype(F32)
    before0 = nn(hot0.astype(BF), upper)
    before1 = nn(hot1.astype(BF), upper) + jnp.sum(hot0, axis=1, keepdims=True)
    pos0 = jnp.sum(hot0 * before0, axis=0, keepdims=True).astype(jnp.int32)
    pos1 = jnp.sum(hot1 * before1, axis=0, keepdims=True).astype(jnp.int32)
    w0, w1 = w_ref[0:1, :], w_ref[1:2, :]
    none = jnp.full_like(ids0, -64)
    a0 = jnp.where(pos0 < MAIN, ids0 * MAIN + pos0, none)
    a1 = jnp.where(pos1 < MAIN, ids1 * MAIN + pos1, none)
    b0 = jnp.where((pos0 >= MAIN) & (pos0 < MAIN + 4), ids0 * MAIN + pos0 - MAIN, none)
    b1 = jnp.where((pos1 >= MAIN) & (pos1 < MAIN + 4), ids1 * MAIN + pos1 - MAIN, none)
    rows_ref[0:1, :] = a0
    rows_ref[1:2, :] = a1
    rows_ref[2:3, :] = b0
    rows_ref[3:4, :] = b1

    def picked(r0, r1, base):
        s0, s1 = selection(r0, base), selection(r1, base)
        weight = jnp.sum(jnp.where(s0, w0, 0.0) + jnp.where(s1, w1, 0.0), axis=1, keepdims=True)
        return (s0 | s1).astype(F32).astype(BF), weight

    sel, weight = picked(a0, a1, 0)
    sel_h, _ = picked(b0, b1, 0)
    sel_s, weight_s = picked(b0, b1, 4)
    for h_in, c_in, to in ((h_ref, c_ref, out_ref), (hd_ref, cd_ref, direct_ref)):
        h, c = h_in[...], c_in[...]
        width = h.shape[1]
        to[:, 0:width] = nn(sel, h).astype(BF)
        to[:, width : 2 * width] = (nn(sel, c) * weight).astype(BF)
        to[:, 2 * width :] = (nn(sel_h, h) + nn(sel_s, c) * weight_s).astype(BF)


def route(tp, ids, weights, hidden_in, cotangent):
    tokens, width = hidden_in.shape
    direct = width // 4
    ring = (width - direct) // 4
    share = pl.BlockSpec((tokens, ring), lambda i, t: (0, t[0]))
    last = pl.BlockSpec((tokens, direct), lambda i, t: (0, 3))
    whole = lambda shape: pl.BlockSpec(shape, lambda i, t: (0, 0))
    return pl.pallas_call(
        route_kernel,
        grid_spec=pltpu.PrefetchScalarGridSpec(
            num_scalar_prefetch=1,
            grid=(1,),
            in_specs=[whole(ids.shape), whole(weights.shape), share, share, last, last],
            out_specs=[whole((64 * MAIN, 3 * ring)), whole((64 * MAIN, 3 * direct)), whole((4, tokens))],
        ),
        out_shape=[
            jax.ShapeDtypeStruct((64 * MAIN, 3 * ring), BF),
            jax.ShapeDtypeStruct((64 * MAIN, 3 * direct), BF),
            jax.ShapeDtypeStruct((4, tokens), jnp.int32),
        ],
        compiler_params=pltpu.CompilerParams(vmem_limit_bytes=VMEM_LIMIT),
        name="route",
    )(tp, ids, weights, hidden_in, cotangent, hidden_in, cotangent)


def combine_kernel(tp_ref, rows_ref, back_ref, c_ref, out_ref):
    width = c_ref.shape[1]
    a0, a1, b0, b1 = (rows_ref[k : k + 1, :] for k in range(4))

    def sel(r0, r1, base):
        return (selection(r0, base) | selection(r1, base)).astype(F32).astype(BF)

    main = tn(sel(a0, a1, 0), back_ref[:, 0:width])
    rest = back_ref[:, width:]
    low = tn(sel(b0, b1, 0), rest)
    high = tn(sel(b0, b1, 4), rest)
    half = width // 2
    out_ref[:, 0:half] = (c_ref[:, 0:half].astype(F32) + (main[:, 0:half] + low)).astype(BF)
    out_ref[:, half:] = (c_ref[:, half:].astype(F32) + (main[:, half:] + high)).astype(BF)


def combine(tp, rows, back, cotangent):
    tokens, width = cotangent.shape[0], cotangent.shape[1] // 4
    whole = lambda shape: pl.BlockSpec(shape, lambda i, t: (0, 0))
    return pl.pallas_call(
        combine_kernel,
        grid_spec=pltpu.PrefetchScalarGridSpec(
            num_scalar_prefetch=1,
            grid=(1,),
            in_specs=[
                whole(rows.shape),
                whole(back.shape),
                pl.BlockSpec((tokens, width), lambda i, t: (0, t[0])),
            ],
            out_specs=whole((tokens, width)),
        ),
        out_shape=jax.ShapeDtypeStruct((tokens, width), BF),
        compiler_params=pltpu.CompilerParams(vmem_limit_bytes=SMALL_LIMIT),
        name="combine",
    )(tp, rows, back, in_hbm(cotangent))


def d_y_kernel(tp_ref, res_ref, wo_own, wo_prev, wo_next, wo_far, dy_own, dy_prev, dy_next, dy_far):
    for w_ref, dy in ((wo_own, dy_own), (wo_prev, dy_prev), (wo_next, dy_next), (wo_far, dy_far)):
        dy[...] = nn(res_ref[...], w_ref[...]).astype(dy.dtype)


def block_at(tp, by):
    return lax.rem(tp + by, 4)


def vmem_specs(n):
    return [pl.BlockSpec(memory_space=pltpu.VMEM) for _ in range(n)]


def in_hbm(x):
    return pltpu.with_memory_space_constraint(x, pltpu.HBM)


def local_call(kernel, scalars, arrays, outs, limit=VMEM_LIMIT):
    return pl.pallas_call(
        kernel,
        in_specs=[pl.BlockSpec(memory_space=pltpu.SMEM)] + vmem_specs(len(arrays)),
        out_specs=vmem_specs(len(outs)),
        out_shape=[jax.ShapeDtypeStruct(shape, dtype) for shape, dtype in outs],
        compiler_params=pltpu.CompilerParams(vmem_limit_bytes=limit),
    )(scalars, *arrays)


def block_rows(tp, by, width):
    return pl.ds(pl.multiple_of(block_at(tp, by) * width, width), width)


def gather_products(sums, lo, x_ref, wg, wu, wd, first):
    ga, ua, da, gb, ub, db = sums
    width = x_ref.shape[1] // 3
    to = slice(lo, lo + x_ref.shape[0])
    h, s, m = x_ref[:, 0:width], x_ref[:, width : 2 * width], x_ref[:, 2 * width :]

    def add(ref, x):
        ref[to, :] = x if first else ref[to, :] + x

    add(ga, nn(h, wg))
    add(ua, nn(h, wu))
    add(da, nt(s, wd))
    add(gb, nn(m, wg))
    add(ub, nn(m, wu))
    add(db, nt(m, wd))


def early_kernel(tp_ref, own_ref, prev_ref, next_ref, wg_ref, wu_ref, wd_ref, *sums):
    tp = tp_ref[0]
    width = own_ref.shape[1] // 3
    for ref, by in ((own_ref, 0), (prev_ref, 3), (next_ref, 1)):
        at = block_rows(tp, by, width)
        gather_products(sums, 0, ref, wg_ref[at, :], wu_ref[at, :], wd_ref[:, at], by == 0)


def partial_rows(da, db, high_p, high_q, wg, wu):
    ff = wg.shape[1]
    cut = wg.shape[0] // 2
    main = nt(da[:, 0:ff], wg) + nt(da[:, ff : 2 * ff], wu)
    rest = nt(db[:, 0:ff], wg[0:cut]) + nt(db[:, ff : 2 * ff], wu[0:cut])
    rest = rest + nt(high_p, wg[cut:]) + nt(high_q, wu[cut:])
    return main.astype(BF), rest.astype(BF)


def write_rows(refs, main, rest):
    at = 0
    for ref in refs:
        n, width = ref.shape[0], main.shape[1]
        ref[:, 0:width] = main[at : at + n]
        ref[:, width:] = rest[at : at + n]
        at += n


def late_kernel(
    tp_ref, ga_in, ua_in, da_in, gb_in, ub_in, db_in, far_lo_in, far_hi_in, direct_in,
    wg_in, wu_in, wd_in, da_out, db_out, far_lo_out, far_hi_out,
    ga, ua, da, gb, ub, db, ga_s, ua_s, da_s, gb_s, ub_s, db_s,
    far, wg_d, wu_d, wd_d, wg_f, wu_f, wd_f, wg_o, wu_o, sems,
):
    tp = tp_ref[0]
    n_rows, ff = ga.shape
    half = n_rows // 2
    width, tail = wg_f.shape[0], wg_d.shape[0]
    last = slice(4 * width, 4 * width + tail)
    opposite = block_rows(tp, 2, width)
    share = block_rows(tp, 2, wg_o.shape[0])
    moves = [
        (wg_in.at[last, :], wg_d), (wu_in.at[last, :], wu_d), (wd_in.at[:, last], wd_d),
        (far_lo_in, far.at[0:half, :]), (far_hi_in, far.at[half:n_rows, :]),
        (wg_in.at[opposite, :], wg_f), (wu_in.at[opposite, :], wu_f), (wd_in.at[:, opposite], wd_f),
        (ga_in, ga_s), (ua_in, ua_s), (da_in, da_s), (gb_in, gb_s), (ub_in, ub_s), (db_in, db_s),
        (wg_in.at[share, :], wg_o), (wu_in.at[share, :], wu_o),
    ]
    copies = [pltpu.make_async_copy(src, dst, sems.at[k]) for k, (src, dst) in enumerate(moves)]
    for copy in copies:
        copy.start()
    sums = (ga, ua, da, gb, ub, db)
    for copy in copies[0:3]:
        copy.wait()
    gather_products(sums, 0, direct_in, wg_d[...], wu_d[...], wd_d[...], True)
    for copy in copies[3:8]:
        copy.wait()
    gather_products(sums, 0, far, wg_f[...], wu_f[...], wd_f[...], False)
    for copy in copies[8:16]:
        copy.wait()

    def local(g, u, d):
        sigma = 1.0 / (1.0 + jnp.exp(-g))
        silu = g * sigma
        return d * u * sigma * (1.0 + g * (1.0 - sigma)), d * silu, silu * u

    p, q, r = local(ga[...] + ga_s[...], ua[...] + ua_s[...], da[...] + da_s[...])
    da_out[:, 0:ff] = p.astype(BF)
    da_out[:, ff : 2 * ff] = q.astype(BF)
    da_out[:, 2 * ff : 3 * ff] = r.astype(BF)
    keep = lax.rem(lax.broadcasted_iota(jnp.int32, (n_rows, ff), 0), 8) < 4
    p, q, r = local(gb[...] + gb_s[...], ub[...] + ub_s[...], pltpu.roll(db[...] + db_s[...], n_rows - 4, 0))
    p, q, r = (jnp.where(keep, v, 0.0) for v in (p, q, r))
    db_out[:, 0:ff] = p.astype(BF)
    db_out[:, ff : 2 * ff] = q.astype(BF)
    db_out[:, 2 * ff : 3 * ff] = pltpu.roll(r, 4, 0).astype(BF)
    db_out[:, 3 * ff : 4 * ff] = pltpu.roll(p, 4, 0).astype(BF)
    db_out[:, 4 * ff :] = pltpu.roll(q, 4, 0).astype(BF)
    high_p, high_q = db_out[:, 3 * ff : 4 * ff], db_out[:, 4 * ff :]
    write_rows((far_lo_out, far_hi_out), *partial_rows(da_out, db_out, high_p, high_q, wg_o[...], wu_o[...]))


def late(tp, sums, far_lo, far_hi, direct, wg, wu, wd):
    n_rows, ff = sums[0].shape
    model = wg.shape[0]
    width, tail = far_lo.shape[1] // 3, direct.shape[1] // 3
    share = model // 4
    piece = jax.ShapeDtypeStruct((n_rows // 2, share + share // 2), BF)
    vmem = pltpu.VMEM
    return pl.pallas_call(
        late_kernel,
        in_specs=[pl.BlockSpec(memory_space=pltpu.SMEM)]
        + [pl.BlockSpec(memory_space=pltpu.HBM)] * 8
        + vmem_specs(1)
        + [pl.BlockSpec(memory_space=pltpu.HBM)] * 3,
        out_specs=vmem_specs(4),
        out_shape=[
            jax.ShapeDtypeStruct((n_rows, 3 * ff), BF), jax.ShapeDtypeStruct((n_rows, 5 * ff), BF), piece, piece,
        ],
        scratch_shapes=[vmem((n_rows, ff), F32)] * 12
        + [vmem((n_rows, 3 * width), BF)]
        + [vmem((tail, ff), BF), vmem((tail, ff), BF), vmem((ff, tail), BF)]
        + [vmem((width, ff), BF), vmem((width, ff), BF), vmem((ff, width), BF)]
        + [vmem((share, ff), BF), vmem((share, ff), BF), pltpu.SemaphoreType.DMA((16,))],
        compiler_params=pltpu.CompilerParams(vmem_limit_bytes=SMALL_LIMIT),
        name="late",
    )(tp, *map(in_hbm, sums), far_lo, far_hi, direct, in_hbm(wg), in_hbm(wu), in_hbm(wd))


def near_kernel(
    tp_ref, da, db, wg_ref, wu_ref, up_lo_out, up_hi_out, down_lo_out, down_hi_out, own_out
):
    tp = tp_ref[0]
    model, ff = wg_ref.shape
    high_p, high_q = db[:, 3 * ff : 4 * ff], db[:, 4 * ff :]
    for by, refs in ((1, (up_lo_out, up_hi_out)), (3, (down_lo_out, down_hi_out)), (0, (own_out,))):
        at = block_rows(tp, by, model // 4)
        write_rows(refs, *partial_rows(da, db, high_p, high_q, wg_ref[at, :], wu_ref[at, :]))


def weights_kernel(
    tp_ref, own_ref, prev_ref, next_ref, far_lo_ref, far_hi_ref, direct_ref, da_ref, db_ref,
    gg_ref, gu_ref, gd_ref,
):
    tp = tp_ref[0]
    width = own_ref.shape[1] // 3
    half = own_ref.shape[0] // 2
    ff, model = gd_ref.shape

    def sums(x_ref, lo):
        n, wide = x_ref.shape[0], x_ref.shape[1] // 3
        da, db = da_ref[lo : lo + n, :], db_ref[lo : lo + n, :]
        h, s, m = x_ref[:, 0:wide], x_ref[:, wide : 2 * wide], x_ref[:, 2 * wide :]
        both = tn(h, da[:, 0 : 2 * ff]) + tn(m, db[:, 0 : 2 * ff])
        down = tn(da[:, 2 * ff : 3 * ff], s) + tn(db[:, 2 * ff : 3 * ff], m)
        return both, down

    def put(at, both, down):
        gg_ref[at, :] = both[:, 0:ff].astype(BF)
        gu_ref[at, :] = both[:, ff:].astype(BF)
        gd_ref[:, at] = down.astype(BF)

    put(block_rows(tp, 0, width), *sums(own_ref, 0))
    put(block_rows(tp, 3, width), *sums(prev_ref, 0))
    put(block_rows(tp, 1, width), *sums(next_ref, 0))
    both, down = sums(far_lo_ref, 0)
    both_hi, down_hi = sums(far_hi_ref, half)
    put(block_rows(tp, 2, width), both + both_hi, down + down_hi)
    put(slice(4 * width, model), *sums(direct_ref, 0))


def mixer_kernel(where_ref, res_ref, res_o_ref, y_ref, y_o_ref, out_ref):
    tp, core = lax.rem(where_ref[0], 4), lax.div(where_ref[0], 4)
    width = res_ref.shape[1]
    chan = out_ref.shape[1]
    for k, by in enumerate((0, 3, 1, 2)):
        at = slice(k * chan, (k + 1) * chan)
        grad = tn(res_ref[...], y_ref[:, at]) + tn(res_o_ref[...], y_o_ref[:, at])
        grad = grad.reshape(width // 64, 2, 32, chan)
        mine = jnp.where(core == 0, grad[:, 0], grad[:, 1]).reshape(width // 2, chan)
        out_ref[block_rows(tp, by + 2, width // 2), :] = mine.astype(BF)


def from_behind(x, by):
    n = lax.axis_size(SP)
    return lax.ppermute(x, SP, [(i, i + by) for i in range(n) if 0 <= i + by < n])


def ring(x):
    half = x.shape[0] // 2
    prev = shifted(x, "y", 1)
    after = shifted(x, "y", -1)
    return prev, after, shifted(prev[:half], "y", 1), shifted(after[half:], "y", -1)


def per_device(
    hidden_in, cotangent, routes, routing_weights, w_gate, w_up, w_down, b_gate, c_gate, x_in, taps, w_out
):
    tok_rows, model_width = hidden_in.shape
    share = model_width // 4
    chan = w_out.shape[1]
    y_at = lax.axis_index("y").astype(jnp.int32)
    tp = y_at.reshape(1)
    where = (y_at + 4 * lax.axis_index("c").astype(jnp.int32)).reshape(1)
    wg, wu, wd = w_gate[0], w_up[0], w_down[0]
    ff = wg.shape[1]

    sent, sent_direct, rows = route(tp, routes.T, routing_weights.T, hidden_in, cotangent)
    to_experts = lambda v: lax.all_to_all(
        v.reshape(64, MAIN, v.shape[1]), SP, split_axis=0, concat_axis=0, tiled=True
    ).reshape(v.shape)
    tail = slice(tok_rows - 2, tok_rows)
    earlier = from_behind(c_gate[tail].astype(F32) * x_in[tail].astype(F32), 1)
    own = to_experts(sent)

    part = lambda by: lax.dynamic_slice_in_dim(w_out, lax.rem(y_at + by, 4) * share, share, 0)
    wo_blocks = (part(0), shifted(part(1), "y", 1), shifted(part(3), "y", -1), shifted(part(2), "y", 2))
    own, sent_direct, *wo_blocks = lax.optimization_barrier((own, sent_direct, *wo_blocks))

    prev, after, far_lo, far_hi = ring(own)
    far_lo, far_hi = in_hbm(far_lo), in_hbm(far_hi)
    direct = to_experts(sent_direct)

    n_rows, half = own.shape[0], own.shape[0] // 2
    out_width = share + share // 2
    sums = local_call(early_kernel, tp, (own, prev, after, wg, wu, wd), [((n_rows, ff), F32)] * 6)
    da, db, f_lo, f_hi = late(tp, sums, far_lo, far_hi, direct, wg, wu, wd)
    u_lo, u_hi, d_lo, d_hi, o = local_call(
        near_kernel, tp, (da, db, in_hbm(wg), in_hbm(wu)),
        [((half, out_width), BF)] * 4 + [((n_rows, out_width), BF)], SMALL_LIMIT,
    )

    from_prev = shifted(f_lo, "y", 1)
    from_next = shifted(f_hi, "y", -1)
    prev_hi = shifted(u_hi, "y", 1)
    next_lo = shifted(d_lo, "y", -1)
    added = lambda a, b: (a.astype(F32) + b.astype(F32)).astype(BF)
    prev_lo = shifted(added(u_lo, from_prev), "y", 1)
    next_hi = shifted(added(d_hi, from_next), "y", -1)
    got_prev = jnp.concatenate([prev_lo, prev_hi], axis=0).astype(F32)
    got_next = jnp.concatenate([next_lo, next_hi], axis=0).astype(F32)
    total = (o.astype(F32) + got_prev + got_next).astype(BF)
    total, earlier = lax.optimization_barrier((total, earlier))
    back = to_experts(total)

    taps_f = taps.astype(F32)
    gated = c_gate.astype(F32) * x_in.astype(F32)
    padded = jnp.concatenate([earlier, gated], axis=0)
    conv = (
        taps_f[0] * padded[0:tok_rows]
        + taps_f[1] * padded[1 : tok_rows + 1]
        + taps_f[2] * padded[2 : tok_rows + 2]
    )
    y_short = (b_gate.astype(F32) * conv).astype(BF)
    y_all = jnp.concatenate(
        (y_short, shifted(y_short, "y", 1), shifted(y_short, "y", -1), shifted(y_short, "y", 2)), axis=1
    )
    y_other = shifted(y_all, "c", 1)
    gg, gu, gd = local_call(
        weights_kernel, tp, (own, prev, after, far_lo, far_hi, direct, da, db),
        [((model_width, ff), BF), ((model_width, ff), BF), ((ff, model_width), BF)],
    )
    back, gg, gu, gd, y_other = lax.optimization_barrier((back, gg, gu, gd, y_other))

    residual_grad = combine(tp, rows, back, cotangent)
    res_other = shifted(residual_grad, "c", 1)
    dy, dy_prev, dy_next, dy_far = local_call(
        d_y_kernel, tp, (in_hbm(residual_grad), *map(in_hbm, wo_blocks)),
        [((tok_rows, chan), F32)] + [((tok_rows, chan), BF)] * 3, SMALL_LIMIT,
    )
    (chip,) = local_call(
        mixer_kernel, where, (in_hbm(residual_grad), res_other, in_hbm(y_all), in_hbm(y_other)),
        [((2 * share, chan), BF)], SMALL_LIMIT,
    )
    d_y = (
        dy
        + shifted(dy_prev, "y", -1).astype(F32)
        + shifted(dy_next, "y", 1).astype(F32)
        + shifted(dy_far, "y", 2).astype(F32)
    )
    grad_b = (d_y * conv).astype(BF)
    d_conv = b_gate.astype(F32) * d_y
    following = from_behind(d_conv[0:2], -1)
    later = jnp.concatenate([d_conv, following], axis=0)
    d_v = (
        taps_f[2] * later[0:tok_rows]
        + taps_f[1] * later[1 : tok_rows + 1]
        + taps_f[0] * later[2 : tok_rows + 2]
    )
    grad_c = (d_v * x_in.astype(F32)).astype(BF)
    grad_x = (d_v * c_gate.astype(F32)).astype(BF)

    parts = lax.all_to_all(chip.reshape(32, 32, chan), ("z", "x"), split_axis=0, concat_axis=0, tiled=True)
    piece = jnp.sum(parts.astype(F32), axis=0)
    at = lambda z, x, c, y: ((z * 4 + x) * 2 + c) * 4 + y
    pairs = [
        (at(z, x, c, y), at(2 * y + z % 2, x, c, (z // 2 + 2) % 4))
        for z in range(8) for x in range(4) for c in range(2) for y in range(4)
    ]
    out_proj_grad = lax.ppermute(piece, ("z", "x", "c", "y"), pairs)

    return (gg[None], gu[None], gd[None], out_proj_grad, residual_grad, grad_b, grad_c, grad_x)


def solution(mesh):
    fine = Mesh(mesh.devices.reshape(8, 4, 2, 4), ("z", "x", "c", "y"))
    rows = P(SP, None)
    both = P(SP, "y")
    return jax.shard_map(
        per_device,
        mesh=fine,
        in_specs=(
            rows, rows, rows, rows,
            P(SP, None, "y"), P(SP, None, "y"), P(SP, "y", None),
            both, both, both, P(None, "y"), P(None, "y"),
        ),
        out_specs=(P(SP, None, "y"), P(SP, None, "y"), P(SP, "y", None), both, both, both, both, both),
        check_vma=False,
    )
```

```python
import jax
import jax.numpy as jnp
from jax import lax
from jax.experimental import pallas as pl
from jax.experimental.pallas import tpu as pltpu
from jax.sharding import Mesh, PartitionSpec as P

BF = jnp.bfloat16
F32 = jnp.float32
SP = ("z", "x", "c")
MAIN = 8
VMEM_LIMIT = 56 * 1024 * 1024
SMALL_LIMIT = 20 * 1024 * 1024


def dot(a, b, contract):
    return lax.dot_general(a, b, ((contract[0], contract[1]), ((), ())), preferred_element_type=F32)


def nn(a, b):
    return dot(a, b, ((1,), (0,)))


def nt(a, b):
    return dot(a, b, ((1,), (1,)))


def tn(a, b):
    return dot(a, b, ((0,), (0,)))


def shifted(x, axis, by):
    n = lax.axis_size(axis)
    return lax.ppermute(x, axis, [(i, (i + by) % n) for i in range(n)])


def selection(row, base=0):
    n_rows = 64 * MAIN
    at = lax.broadcasted_iota(jnp.int32, (n_rows, row.shape[1]), 0)
    return at == (row + base)


def picked(r0, r1, w0, w1, base):
    s0, s1 = selection(r0, base), selection(r1, base)
    weight = jnp.sum(jnp.where(s0, w0, 0.0) + jnp.where(s1, w1, 0.0), axis=1, keepdims=True)
    return (s0 | s1).astype(F32).astype(BF), weight


def select_rows(a0, a1, b0, b1, w_ref, h_ref, c_ref, out_ref):
    w0, w1 = w_ref[0:1, :], w_ref[1:2, :]
    sel, weight = picked(a0, a1, w0, w1, 0)
    sel_h, _ = picked(b0, b1, w0, w1, 0)
    sel_s, weight_s = picked(b0, b1, w0, w1, 4)
    h, c = h_ref[...], c_ref[...]
    width = h.shape[1]
    out_ref[:, 0:width] = nn(sel, h).astype(BF)
    out_ref[:, width : 2 * width] = (nn(sel, c) * weight).astype(BF)
    out_ref[:, 2 * width :] = (nn(sel_h, h) + nn(sel_s, c) * weight_s).astype(BF)


def route_kernel(tp_ref, ids_ref, w_ref, h_ref, c_ref, out_ref, rows_ref):
    tokens = ids_ref.shape[1]
    expert = lax.broadcasted_iota(jnp.int32, (64, tokens), 0)
    upper = (
        lax.broadcasted_iota(jnp.int32, (tokens, tokens), 0)
        < lax.broadcasted_iota(jnp.int32, (tokens, tokens), 1)
    ).astype(F32).astype(BF)
    ids0, ids1 = ids_ref[0:1, :], ids_ref[1:2, :]
    hot0 = (expert == ids0).astype(F32)
    hot1 = (expert == ids1).astype(F32)
    before0 = nn(hot0.astype(BF), upper)
    before1 = nn(hot1.astype(BF), upper) + jnp.sum(hot0, axis=1, keepdims=True)
    pos0 = jnp.sum(hot0 * before0, axis=0, keepdims=True).astype(jnp.int32)
    pos1 = jnp.sum(hot1 * before1, axis=0, keepdims=True).astype(jnp.int32)
    none = jnp.full_like(ids0, -64)
    a0 = jnp.where(pos0 < MAIN, ids0 * MAIN + pos0, none)
    a1 = jnp.where(pos1 < MAIN, ids1 * MAIN + pos1, none)
    b0 = jnp.where((pos0 >= MAIN) & (pos0 < MAIN + 4), ids0 * MAIN + pos0 - MAIN, none)
    b1 = jnp.where((pos1 >= MAIN) & (pos1 < MAIN + 4), ids1 * MAIN + pos1 - MAIN, none)
    rows_ref[0:1, :] = a0
    rows_ref[1:2, :] = a1
    rows_ref[2:3, :] = b0
    rows_ref[3:4, :] = b1
    select_rows(a0, a1, b0, b1, w_ref, h_ref, c_ref, out_ref)


def direct_kernel(rows_ref, w_ref, h_ref, c_ref, out_ref):
    select_rows(*(rows_ref[k : k + 1, :] for k in range(4)), w_ref, h_ref, c_ref, out_ref)


def route(tp, ids, weights, hidden_in, cotangent):
    tokens, width = hidden_in.shape
    ring = 3 * width // 16
    share = pl.BlockSpec((tokens, ring), lambda i, t: (0, t[0]))
    whole = lambda shape: pl.BlockSpec(shape, lambda i, t: (0, 0))
    return pl.pallas_call(
        route_kernel,
        grid_spec=pltpu.PrefetchScalarGridSpec(
            num_scalar_prefetch=1,
            grid=(1,),
            in_specs=[whole(ids.shape), whole(weights.shape), share, share],
            out_specs=[whole((64 * MAIN, 3 * ring)), whole((4, tokens))],
        ),
        out_shape=[
            jax.ShapeDtypeStruct((64 * MAIN, 3 * ring), BF),
            jax.ShapeDtypeStruct((4, tokens), jnp.int32),
        ],
        compiler_params=pltpu.CompilerParams(vmem_limit_bytes=VMEM_LIMIT),
        name="route",
    )(tp, ids, weights, hidden_in, cotangent)


def route_direct(rows, weights, hidden_in, cotangent):
    tokens, width = hidden_in.shape
    direct = width // 4
    last = pl.BlockSpec((tokens, direct), lambda i: (0, 3))
    whole = lambda shape: pl.BlockSpec(shape, lambda i: (0, 0))
    return pl.pallas_call(
        direct_kernel,
        grid=(1,),
        in_specs=[whole(rows.shape), whole(weights.shape), last, last],
        out_specs=whole((64 * MAIN, 3 * direct)),
        out_shape=jax.ShapeDtypeStruct((64 * MAIN, 3 * direct), BF),
        compiler_params=pltpu.CompilerParams(vmem_limit_bytes=VMEM_LIMIT),
        name="route_direct",
    )(rows, weights, hidden_in, cotangent)


def combine_kernel(tp_ref, rows_ref, back_ref, c_ref, out_ref):
    width = c_ref.shape[1]
    a0, a1, b0, b1 = (rows_ref[k : k + 1, :] for k in range(4))

    def sel(r0, r1, base):
        return (selection(r0, base) | selection(r1, base)).astype(F32).astype(BF)

    main = tn(sel(a0, a1, 0), back_ref[:, 0:width])
    rest = back_ref[:, width:]
    low = tn(sel(b0, b1, 0), rest)
    high = tn(sel(b0, b1, 4), rest)
    half = width // 2
    out_ref[:, 0:half] = (c_ref[:, 0:half].astype(F32) + (main[:, 0:half] + low)).astype(BF)
    out_ref[:, half:] = (c_ref[:, half:].astype(F32) + (main[:, half:] + high)).astype(BF)


def combine(tp, rows, back, cotangent):
    tokens, width = cotangent.shape[0], cotangent.shape[1] // 4
    whole = lambda shape: pl.BlockSpec(shape, lambda i, t: (0, 0))
    return pl.pallas_call(
        combine_kernel,
        grid_spec=pltpu.PrefetchScalarGridSpec(
            num_scalar_prefetch=1,
            grid=(1,),
            in_specs=[
                whole(rows.shape),
                whole(back.shape),
                pl.BlockSpec((tokens, width), lambda i, t: (0, t[0])),
            ],
            out_specs=whole((tokens, width)),
        ),
        out_shape=jax.ShapeDtypeStruct((tokens, width), BF),
        compiler_params=pltpu.CompilerParams(vmem_limit_bytes=SMALL_LIMIT),
        name="combine",
    )(tp, rows, back, in_hbm(cotangent))


def d_y_kernel(tp_ref, res_ref, wo_own, wo_prev, wo_next, wo_far, dy_own, dy_prev, dy_next, dy_far):
    for w_ref, dy in ((wo_own, dy_own), (wo_prev, dy_prev), (wo_next, dy_next), (wo_far, dy_far)):
        dy[...] = nn(res_ref[...], w_ref[...]).astype(dy.dtype)


def block_at(tp, by):
    return lax.rem(tp + by, 4)


def vmem_specs(n):
    return [pl.BlockSpec(memory_space=pltpu.VMEM) for _ in range(n)]


def in_hbm(x):
    return pltpu.with_memory_space_constraint(x, pltpu.HBM)


def local_call(kernel, scalars, arrays, outs, limit=VMEM_LIMIT):
    return pl.pallas_call(
        kernel,
        in_specs=[pl.BlockSpec(memory_space=pltpu.SMEM)] + vmem_specs(len(arrays)),
        out_specs=vmem_specs(len(outs)),
        out_shape=[jax.ShapeDtypeStruct(shape, dtype) for shape, dtype in outs],
        compiler_params=pltpu.CompilerParams(vmem_limit_bytes=limit),
    )(scalars, *arrays)


def block_rows(tp, by, width):
    return pl.ds(pl.multiple_of(block_at(tp, by) * width, width), width)


def gather_products(sums, lo, x_ref, wg, wu, wd, first):
    ga, ua, da, gb, ub, db = sums
    width = x_ref.shape[1] // 3
    to = slice(lo, lo + x_ref.shape[0])
    h, s, m = x_ref[:, 0:width], x_ref[:, width : 2 * width], x_ref[:, 2 * width :]

    def add(ref, x):
        ref[to, :] = x if first else ref[to, :] + x

    add(ga, nn(h, wg))
    add(ua, nn(h, wu))
    add(da, nt(s, wd))
    add(gb, nn(m, wg))
    add(ub, nn(m, wu))
    add(db, nt(m, wd))


def early_kernel(tp_ref, own_ref, prev_ref, next_ref, wg_ref, wu_ref, wd_ref, *sums):
    tp = tp_ref[0]
    width = own_ref.shape[1] // 3
    for ref, by in ((own_ref, 0), (prev_ref, 3), (next_ref, 1)):
        at = block_rows(tp, by, width)
        gather_products(sums, 0, ref, wg_ref[at, :], wu_ref[at, :], wd_ref[:, at], by == 0)


def partial_rows(da, db, high_p, high_q, wg, wu):
    ff = wg.shape[1]
    cut = wg.shape[0] // 2
    main = nt(da[:, 0:ff], wg) + nt(da[:, ff : 2 * ff], wu)
    rest = nt(db[:, 0:ff], wg[0:cut]) + nt(db[:, ff : 2 * ff], wu[0:cut])
    rest = rest + nt(high_p, wg[cut:]) + nt(high_q, wu[cut:])
    return main.astype(BF), rest.astype(BF)


def write_rows(refs, main, rest):
    at = 0
    for ref in refs:
        n, width = ref.shape[0], main.shape[1]
        ref[:, 0:width] = main[at : at + n]
        ref[:, width:] = rest[at : at + n]
        at += n


def late_kernel(
    tp_ref, ga_in, ua_in, da_in, gb_in, ub_in, db_in, far_lo_in, far_hi_in, direct_in,
    wg_in, wu_in, wd_in, da_out, db_out, far_lo_out, far_hi_out,
    ga, ua, da, gb, ub, db, ga_s, ua_s, da_s, gb_s, ub_s, db_s,
    far, wg_d, wu_d, wd_d, wg_f, wu_f, wd_f, wg_o, wu_o, sems,
):
    tp = tp_ref[0]
    n_rows, ff = ga.shape
    half = n_rows // 2
    width, tail = wg_f.shape[0], wg_d.shape[0]
    last = slice(4 * width, 4 * width + tail)
    opposite = block_rows(tp, 2, width)
    share = block_rows(tp, 2, wg_o.shape[0])
    moves = [
        (wg_in.at[last, :], wg_d), (wu_in.at[last, :], wu_d), (wd_in.at[:, last], wd_d),
        (far_lo_in, far.at[0:half, :]), (far_hi_in, far.at[half:n_rows, :]),
        (wg_in.at[opposite, :], wg_f), (wu_in.at[opposite, :], wu_f), (wd_in.at[:, opposite], wd_f),
        (ga_in, ga_s), (ua_in, ua_s), (da_in, da_s), (gb_in, gb_s), (ub_in, ub_s), (db_in, db_s),
        (wg_in.at[share, :], wg_o), (wu_in.at[share, :], wu_o),
    ]
    copies = [pltpu.make_async_copy(src, dst, sems.at[k]) for k, (src, dst) in enumerate(moves)]
    for copy in copies:
        copy.start()
    sums = (ga, ua, da, gb, ub, db)
    for copy in copies[0:3]:
        copy.wait()
    gather_products(sums, 0, direct_in, wg_d[...], wu_d[...], wd_d[...], True)
    for copy in copies[3:8]:
        copy.wait()
    gather_products(sums, 0, far, wg_f[...], wu_f[...], wd_f[...], False)
    for copy in copies[8:16]:
        copy.wait()

    def local(g, u, d):
        sigma = 1.0 / (1.0 + jnp.exp(-g))
        silu = g * sigma
        return d * u * sigma * (1.0 + g * (1.0 - sigma)), d * silu, silu * u

    p, q, r = local(ga[...] + ga_s[...], ua[...] + ua_s[...], da[...] + da_s[...])
    da_out[:, 0:ff] = p.astype(BF)
    da_out[:, ff : 2 * ff] = q.astype(BF)
    da_out[:, 2 * ff : 3 * ff] = r.astype(BF)
    keep = lax.rem(lax.broadcasted_iota(jnp.int32, (n_rows, ff), 0), 8) < 4
    p, q, r = local(gb[...] + gb_s[...], ub[...] + ub_s[...], pltpu.roll(db[...] + db_s[...], n_rows - 4, 0))
    p, q, r = (jnp.where(keep, v, 0.0) for v in (p, q, r))
    db_out[:, 0:ff] = p.astype(BF)
    db_out[:, ff : 2 * ff] = q.astype(BF)
    db_out[:, 2 * ff : 3 * ff] = pltpu.roll(r, 4, 0).astype(BF)
    db_out[:, 3 * ff : 4 * ff] = pltpu.roll(p, 4, 0).astype(BF)
    db_out[:, 4 * ff :] = pltpu.roll(q, 4, 0).astype(BF)
    high_p, high_q = db_out[:, 3 * ff : 4 * ff], db_out[:, 4 * ff :]
    write_rows((far_lo_out, far_hi_out), *partial_rows(da_out, db_out, high_p, high_q, wg_o[...], wu_o[...]))


def late(tp, sums, far_lo, far_hi, direct, wg, wu, wd):
    n_rows, ff = sums[0].shape
    model = wg.shape[0]
    width, tail = far_lo.shape[1] // 3, direct.shape[1] // 3
    share = model // 4
    piece = jax.ShapeDtypeStruct((n_rows // 2, share + share // 2), BF)
    vmem = pltpu.VMEM
    return pl.pallas_call(
        late_kernel,
        in_specs=[pl.BlockSpec(memory_space=pltpu.SMEM)]
        + [pl.BlockSpec(memory_space=pltpu.HBM)] * 8
        + vmem_specs(1)
        + [pl.BlockSpec(memory_space=pltpu.HBM)] * 3,
        out_specs=vmem_specs(4),
        out_shape=[
            jax.ShapeDtypeStruct((n_rows, 3 * ff), BF), jax.ShapeDtypeStruct((n_rows, 5 * ff), BF), piece, piece,
        ],
        scratch_shapes=[vmem((n_rows, ff), F32)] * 12
        + [vmem((n_rows, 3 * width), BF)]
        + [vmem((tail, ff), BF), vmem((tail, ff), BF), vmem((ff, tail), BF)]
        + [vmem((width, ff), BF), vmem((width, ff), BF), vmem((ff, width), BF)]
        + [vmem((share, ff), BF), vmem((share, ff), BF), pltpu.SemaphoreType.DMA((16,))],
        compiler_params=pltpu.CompilerParams(vmem_limit_bytes=SMALL_LIMIT),
        name="late",
    )(tp, *map(in_hbm, sums), far_lo, far_hi, direct, in_hbm(wg), in_hbm(wu), in_hbm(wd))


def near_kernel(
    tp_ref, da, db, wg_ref, wu_ref, up_lo_out, up_hi_out, down_lo_out, down_hi_out, own_out
):
    tp = tp_ref[0]
    model, ff = wg_ref.shape
    high_p, high_q = db[:, 3 * ff : 4 * ff], db[:, 4 * ff :]
    for by, refs in ((1, (up_lo_out, up_hi_out)), (3, (down_lo_out, down_hi_out)), (0, (own_out,))):
        at = block_rows(tp, by, model // 4)
        write_rows(refs, *partial_rows(da, db, high_p, high_q, wg_ref[at, :], wu_ref[at, :]))


def weights_kernel(
    tp_ref, own_ref, prev_ref, next_ref, far_lo_ref, far_hi_ref, direct_ref, da_ref, db_ref,
    gg_ref, gu_ref, gd_ref,
):
    tp = tp_ref[0]
    width = own_ref.shape[1] // 3
    half = own_ref.shape[0] // 2
    ff, model = gd_ref.shape

    def sums(x_ref, lo):
        n, wide = x_ref.shape[0], x_ref.shape[1] // 3
        da, db = da_ref[lo : lo + n, :], db_ref[lo : lo + n, :]
        h, s, m = x_ref[:, 0:wide], x_ref[:, wide : 2 * wide], x_ref[:, 2 * wide :]
        both = tn(h, da[:, 0 : 2 * ff]) + tn(m, db[:, 0 : 2 * ff])
        down = tn(da[:, 2 * ff : 3 * ff], s) + tn(db[:, 2 * ff : 3 * ff], m)
        return both, down

    def put(at, both, down):
        gg_ref[at, :] = both[:, 0:ff].astype(BF)
        gu_ref[at, :] = both[:, ff:].astype(BF)
        gd_ref[:, at] = down.astype(BF)

    put(block_rows(tp, 0, width), *sums(own_ref, 0))
    put(block_rows(tp, 3, width), *sums(prev_ref, 0))
    put(block_rows(tp, 1, width), *sums(next_ref, 0))
    both, down = sums(far_lo_ref, 0)
    both_hi, down_hi = sums(far_hi_ref, half)
    put(block_rows(tp, 2, width), both + both_hi, down + down_hi)
    put(slice(4 * width, model), *sums(direct_ref, 0))


def mixer_kernel(where_ref, res_ref, res_o_ref, y_ref, y_o_ref, out_ref):
    tp, core = lax.rem(where_ref[0], 4), lax.div(where_ref[0], 4)
    width = res_ref.shape[1]
    chan = out_ref.shape[1]

    def rows_of_core(ref):
        turned = ref[...].astype(F32).T.reshape(width // 64, 2, 32, ref.shape[0])
        return jnp.where(core == 0, turned[:, 0], turned[:, 1]).reshape(width // 2, ref.shape[0]).astype(BF)

    mine, other = rows_of_core(res_ref), rows_of_core(res_o_ref)
    for k, by in enumerate((0, 3, 1, 2)):
        at = slice(k * chan, (k + 1) * chan)
        grad = nn(mine, y_ref[:, at]) + nn(other, y_o_ref[:, at])
        out_ref[block_rows(tp, by + 2, width // 2), :] = grad.astype(BF)


def from_behind(x, by):
    n = lax.axis_size(SP)
    return lax.ppermute(x, SP, [(i, i + by) for i in range(n) if 0 <= i + by < n])


def ring(x):
    half = x.shape[0] // 2
    prev = shifted(x, "y", 1)
    after = shifted(x, "y", -1)
    return prev, after, shifted(prev[:half], "y", 1), shifted(after[half:], "y", -1)


def per_device(
    hidden_in, cotangent, routes, routing_weights, w_gate, w_up, w_down, b_gate, c_gate, x_in, taps, w_out
):
    tok_rows, model_width = hidden_in.shape
    share = model_width // 4
    chan = w_out.shape[1]
    y_at = lax.axis_index("y").astype(jnp.int32)
    tp = y_at.reshape(1)
    where = (y_at + 4 * lax.axis_index("c").astype(jnp.int32)).reshape(1)
    wg, wu, wd = w_gate[0], w_up[0], w_down[0]
    ff = wg.shape[1]

    sent, rows = route(tp, routes.T, routing_weights.T, hidden_in, cotangent)
    to_experts = lambda v: lax.all_to_all(
        v.reshape(64, MAIN, v.shape[1]), SP, split_axis=0, concat_axis=0, tiled=True
    ).reshape(v.shape)
    tail = slice(tok_rows - 2, tok_rows)
    earlier = from_behind(c_gate[tail].astype(F32) * x_in[tail].astype(F32), 1)
    own = to_experts(sent)

    part = lambda by: lax.dynamic_slice_in_dim(w_out, lax.rem(y_at + by, 4) * share, share, 0)
    wo_blocks = (part(0), shifted(part(1), "y", 1), shifted(part(3), "y", -1), shifted(part(2), "y", 2))
    sent_direct = route_direct(rows, routing_weights.T, hidden_in, cotangent)
    own, sent_direct, *wo_blocks = lax.optimization_barrier((own, sent_direct, *wo_blocks))

    prev, after, far_lo, far_hi = ring(own)
    far_lo, far_hi = in_hbm(far_lo), in_hbm(far_hi)
    direct = to_experts(sent_direct)

    n_rows, half = own.shape[0], own.shape[0] // 2
    out_width = share + share // 2
    sums = local_call(early_kernel, tp, (own, prev, after, wg, wu, wd), [((n_rows, ff), F32)] * 6)
    da, db, f_lo, f_hi = late(tp, sums, far_lo, far_hi, direct, wg, wu, wd)
    u_lo, u_hi, d_lo, d_hi, o = local_call(
        near_kernel, tp, (da, db, in_hbm(wg), in_hbm(wu)),
        [((half, out_width), BF)] * 4 + [((n_rows, out_width), BF)], SMALL_LIMIT,
    )

    from_prev = shifted(f_lo, "y", 1)
    from_next = shifted(f_hi, "y", -1)
    prev_hi = shifted(u_hi, "y", 1)
    next_lo = shifted(d_lo, "y", -1)
    added = lambda a, b: (a.astype(F32) + b.astype(F32)).astype(BF)
    prev_lo = shifted(added(u_lo, from_prev), "y", 1)
    next_hi = shifted(added(d_hi, from_next), "y", -1)
    got_prev = jnp.concatenate([prev_lo, prev_hi], axis=0).astype(F32)
    got_next = jnp.concatenate([next_lo, next_hi], axis=0).astype(F32)
    total = (o.astype(F32) + got_prev + got_next).astype(BF)
    total, earlier = lax.optimization_barrier((total, earlier))
    back = to_experts(total)

    taps_f = taps.astype(F32)
    gated = c_gate.astype(F32) * x_in.astype(F32)
    padded = jnp.concatenate([earlier, gated], axis=0)
    conv = (
        taps_f[0] * padded[0:tok_rows]
        + taps_f[1] * padded[1 : tok_rows + 1]
        + taps_f[2] * padded[2 : tok_rows + 2]
    )
    y_short = (b_gate.astype(F32) * conv).astype(BF)
    y_all = jnp.concatenate(
        (y_short, shifted(y_short, "y", 1), shifted(y_short, "y", -1), shifted(y_short, "y", 2)), axis=1
    )
    y_other = shifted(y_all, "c", 1)
    gg, gu, gd = local_call(
        weights_kernel, tp, (own, prev, after, far_lo, far_hi, direct, da, db),
        [((model_width, ff), BF), ((model_width, ff), BF), ((ff, model_width), BF)],
    )
    back, gg, gu, gd, y_other = lax.optimization_barrier((back, gg, gu, gd, y_other))

    residual_grad = combine(tp, rows, back, cotangent)
    res_other = shifted(residual_grad, "c", 1)
    dy, dy_prev, dy_next, dy_far = local_call(
        d_y_kernel, tp, (in_hbm(residual_grad), *map(in_hbm, wo_blocks)),
        [((tok_rows, chan), F32)] + [((tok_rows, chan), BF)] * 3, SMALL_LIMIT,
    )
    res_other, dy, dy_prev, dy_next, dy_far = lax.optimization_barrier((res_other, dy, dy_prev, dy_next, dy_far))
    (chip,) = local_call(
        mixer_kernel, where, (in_hbm(residual_grad), res_other, in_hbm(y_all), in_hbm(y_other)),
        [((2 * share, chan), BF)], SMALL_LIMIT,
    )
    d_y = (
        dy
        + shifted(dy_prev, "y", -1).astype(F32)
        + shifted(dy_next, "y", 1).astype(F32)
        + shifted(dy_far, "y", 2).astype(F32)
    )
    grad_b = (d_y * conv).astype(BF)
    d_conv = b_gate.astype(F32) * d_y
    following = from_behind(d_conv[0:2], -1)
    parts = lax.all_to_all(chip.reshape(32, 32, chan), ("z", "x"), split_axis=0, concat_axis=0, tiled=True)
    piece = jnp.sum(parts.astype(F32), axis=0)
    following, piece = lax.optimization_barrier((following, piece))
    at = lambda z, x, c, y: ((z * 4 + x) * 2 + c) * 4 + y
    pairs = [
        (at(z, x, c, y), at(2 * y + z % 2, x, c, (z // 2 + 2) % 4))
        for z in range(8) for x in range(4) for c in range(2) for y in range(4)
    ]
    out_proj_grad = lax.ppermute(piece, ("z", "x", "c", "y"), pairs)

    later = jnp.concatenate([d_conv, following], axis=0)
    d_v = (
        taps_f[2] * later[0:tok_rows]
        + taps_f[1] * later[1 : tok_rows + 1]
        + taps_f[0] * later[2 : tok_rows + 2]
    )
    grad_c = (d_v * x_in.astype(F32)).astype(BF)
    grad_x = (d_v * c_gate.astype(F32)).astype(BF)
    return (gg[None], gu[None], gd[None], out_proj_grad, residual_grad, grad_b, grad_c, grad_x)


def solution(mesh):
    fine = Mesh(mesh.devices.reshape(8, 4, 2, 4), ("z", "x", "c", "y"))
    rows = P(SP, None)
    both = P(SP, "y")
    return jax.shard_map(
        per_device,
        mesh=fine,
        in_specs=(
            rows, rows, rows, rows,
            P(SP, None, "y"), P(SP, None, "y"), P(SP, "y", None),
            both, both, both, P(None, "y"), P(None, "y"),
        ),
        out_specs=(P(SP, None, "y"), P(SP, None, "y"), P(SP, "y", None), both, both, both, both, both),
        check_vma=False,
    )
```
